512 devices in a mesh: sp: 32 (over z, x), tp: 16 (over y, core).
Axes of the slice: x: 4, y: 8, z: 8, core: 2. Of those that a mesh axis runs over, the one named last changes fastest.
Arguments:
- target: bfloat16 [4096, 4096], P('sp', 'tp'), may hold values from -300 to 300
- gain: float32 [4096], P('tp'), may hold values from 0.1 to 1.9
- w_query: bfloat16 [4096, 4096], P('tp'), may hold values from -0.09375 to 0.09375
- queries: bfloat16 [4096, 4096], P('sp', 'tp'), may hold values from -13 to 13
- keys: bfloat16 [16384, 1024], P('sp'), may hold values from -4 to 4
- values: bfloat16 [16384, 1024], P('sp'), may hold values from -4 to 4
- attn_out: bfloat16 [4096, 4096], P('sp', 'tp'), may hold values from -4 to 4
- grad_out: bfloat16 [4096, 4096], P('sp', 'tp'), may hold values from -64 to 64
Outputs:
- grad_rows: bfloat16 [4096, 4096], P('sp', 'tp')
- grad_weight: float32 [4096, 4096], P(('tp', 'sp'))
- grad_keys: float32 [16384, 1024], P(('sp', 'tp'))
- grad_values: float32 [16384, 1024], P(('sp', 'tp'))
The draws below stay inside these ranges and needn't reach their ends.
All inputs are finite; a program needn't handle non-finite values.
Results may differ from the reference program's by a relative error of at most 0.018.
Values may be sent and summed in bfloat16 or wider, within the bound.
No kernel may reach another device: no remote copies, remote signals or barrier semaphores. Data moves between devices by JAX's collectives and lax.ppermute only.
A program may use at most 64 MiB of HBM per device.

```python
import math
import jax
import jax.numpy as jnp
from jax import lax

WIDTH = 4096
HEADS = 16
KV_HEADS = 4
HEAD_DIM = 256
TARGET_ROWS = 4096
SOURCE_ROWS = 16384


def draw_target(key, part):
    base_key = jax.random.fold_in(key, 11)
    row_key = jax.random.fold_in(key, 12)
    col_key = jax.random.fold_in(key, 13)
    array_shape = (TARGET_ROWS, WIDTH)
    base_draw = jnp.clip(jax.random.normal(base_key, array_shape, jnp.float32), -4.0, 4.0)
    row_scale = jnp.exp(jax.random.uniform(row_key, (TARGET_ROWS, 1), jnp.float32, 0.0, math.log(10.0)))
    column_ramp = jnp.exp(math.log(5.0) * jnp.arange(WIDTH, dtype=jnp.float32) / WIDTH)
    col_scale = column_ramp * jax.random.uniform(col_key, (WIDTH,), jnp.float32, 0.5, 1.5)
    return (base_draw * row_scale * col_scale).astype(jnp.bfloat16)


def draw_keys(key, part):
    base_key = jax.random.fold_in(key, 21)
    array_shape = (SOURCE_ROWS, KV_HEADS * HEAD_DIM)
    drawn = jnp.clip(jax.random.normal(base_key, array_shape, jnp.float32), -4.0, 4.0)
    return drawn.astype(jnp.bfloat16)


def draw_queries(key, part):
    base_key = jax.random.fold_in(key, 31)
    array_shape = (TARGET_ROWS, HEADS * HEAD_DIM)
    drawn = jnp.clip(jax.random.normal(base_key, array_shape, jnp.float32), -4.0, 4.0)
    return drawn.astype(jnp.bfloat16)


def steps_of(stream_key, shape, cuts, low, top_value):
    level, own = 1.0, jax.random.fold_in(stream_key, 6)
    for axis_at, shards_of in cuts:
        heights = jnp.exp(jax.random.uniform(jax.random.fold_in(own, axis_at), (shards_of,), jnp.float32, low / len(cuts), top_value / len(cuts)))
        level = level * jnp.repeat(heights, shape[axis_at] // shards_of).reshape([-1 if axis == axis_at else 1 for axis in range(len(shape))])
    return level


def scatter_about(own_key, dims, scale, limit, shards=(), held_as=jnp.bfloat16):
    level = steps_of(own_key, dims, shards, -0.22, 0.18) if shards else 1.0
    values = jax.random.normal(own_key, dims, jnp.float32) * scale * level
    return jnp.minimum(jnp.maximum(values, -limit), limit).astype(held_as)


def setup_inputs(seed: int = 0) -> dict:
    seeds = jax.random.split(jax.random.key(seed), 9)
    return {
        "target": draw_target(jax.random.fold_in(seeds[8], 71), 0),
        "gain": jnp.clip(1.0 + 0.18 * jax.random.normal(seeds[1], (WIDTH,), jnp.float32), 0.1, 1.9),
        "w_query": scatter_about(seeds[2], (WIDTH, HEADS * HEAD_DIM), WIDTH ** -0.5, 0.09375, ((0, 16),)),
        "queries": draw_queries(jax.random.fold_in(seeds[8], 71), 0),
        "keys": draw_keys(jax.random.fold_in(seeds[8], 71), 0),
        "values": scatter_about(seeds[5], (SOURCE_ROWS, KV_HEADS * HEAD_DIM), 1.0, 4.0, ((0, 32),)),
        "attn_out": scatter_about(seeds[6], (TARGET_ROWS, HEADS * HEAD_DIM), 1.0, 4.0, ((0, 32), (1, 16))),
        "grad_out": scatter_about(seeds[7], (TARGET_ROWS, HEADS * HEAD_DIM), 16.0, 64.0, ((0, 32), (1, 16))),
    }


norm_eps = 1e-06

def reference(target, gain, w_query, queries, keys, values, attn_out, grad_out):
    target_wide = target.astype(jnp.float32)
    inverse = lax.rsqrt(lax.optimization_barrier(jnp.mean(target_wide * target_wide, axis=1)) + norm_eps)
    normed = (target_wide * inverse[:, None] * gain).astype(jnp.bfloat16)
    group_size = HEADS // KV_HEADS
    score_scale = HEAD_DIM ** (-0.5)
    row_count = queries.shape[0]
    source_count = keys.shape[0]
    query_heads = queries.reshape(row_count, HEADS, HEAD_DIM).transpose(1, 0, 2)
    grad_heads = grad_out.reshape(row_count, HEADS, HEAD_DIM).transpose(1, 0, 2)
    out_heads = attn_out.reshape(row_count, HEADS, HEAD_DIM).transpose(1, 0, 2)
    deltas = lax.optimization_barrier(jnp.sum(grad_heads.astype(jnp.float32) * out_heads.astype(jnp.float32), axis=2))
    head_ids = jnp.arange(HEADS, dtype=jnp.int32)

    def one_head(inputs):
        query_head, grad_head, delta_head, head_id = inputs
        kv_start = (head_id // group_size * HEAD_DIM).astype(jnp.int32)
        key_head = lax.dynamic_slice_in_dim(keys, kv_start, HEAD_DIM, 1)
        value_head = lax.dynamic_slice_in_dim(values, kv_start, HEAD_DIM, 1)
        scores = jnp.dot(query_head, key_head.T, preferred_element_type=jnp.float32) * score_scale
        row_peak = lax.optimization_barrier(jnp.max(scores, axis=1))
        log_totals = row_peak + jnp.log(lax.optimization_barrier(jnp.sum(jnp.exp(scores - row_peak[:, None]), axis=1)))
        weights = jnp.exp(scores - log_totals[:, None])
        weights_rounded = weights.astype(jnp.bfloat16)
        grad_weights = jnp.dot(grad_head, value_head.T, preferred_element_type=jnp.float32)
        grad_scores = (weights * (grad_weights - delta_head[:, None]) * score_scale).astype(jnp.bfloat16)
        query_part = jnp.dot(grad_scores, key_head, preferred_element_type=jnp.float32)
        key_part = jnp.dot(grad_scores.T, query_head, preferred_element_type=jnp.float32)
        value_part = jnp.dot(weights_rounded.T, grad_head, preferred_element_type=jnp.float32)
        return (query_part, key_part, value_part)
    query_parts, key_parts, value_parts = lax.map(one_head, (query_heads, grad_heads, deltas, head_ids))
    query_grad = query_parts.astype(jnp.bfloat16).transpose(1, 0, 2).reshape(row_count, HEADS * HEAD_DIM)
    grad_keys = key_parts.reshape(KV_HEADS, group_size, source_count, HEAD_DIM).sum(axis=1)
    grad_keys = grad_keys.transpose(1, 0, 2).reshape(source_count, KV_HEADS * HEAD_DIM)
    grad_values = value_parts.reshape(KV_HEADS, group_size, source_count, HEAD_DIM).sum(axis=1)
    grad_values = grad_values.transpose(1, 0, 2).reshape(source_count, KV_HEADS * HEAD_DIM)
    grad_rows = jnp.dot(query_grad, w_query.T, preferred_element_type=jnp.float32).astype(jnp.bfloat16)
    grad_weight = jnp.dot(normed.T, query_grad, preferred_element_type=jnp.float32)
    return (grad_rows, grad_weight, grad_keys, grad_values)
```

```python
import jax
import jax.numpy as jnp
from jax import lax
from jax.sharding import Mesh
from jax.sharding import PartitionSpec as P

WIDTH = 4096
HEADS = 16
KV_HEADS = 4
HEAD_DIM = 256
EPS = 1e-06
SCALE = HEAD_DIM ** (-0.5)
F32 = jnp.float32
BF16 = jnp.bfloat16


def shifted(value, axis, by):
    n = lax.axis_size(axis)
    return lax.ppermute(value, axis, [(i, (i + by) % n) for i in range(n)])


def told_all(value, axis):
    n = lax.axis_size(axis)
    sent = jnp.broadcast_to(value[None], (n, *value.shape))
    return lax.all_to_all(sent, axis, split_axis=0, concat_axis=0, tiled=True)


def exchanged(value, axis):
    return lax.all_to_all(value, axis, split_axis=0, concat_axis=0, tiled=True)


def dot(a, b, ca, cb):
    return lax.dot_general(a, b, (((ca,), (cb,)), ((), ())), preferred_element_type=F32)


def local(target, gain, w_query, queries, keys, values, attn_out, grad_out):
    nz, nx = lax.axis_size("z"), lax.axis_size("x")
    rows, cols = queries.shape
    src = keys.shape[0]
    core = lax.axis_index("c")
    x_at = lax.axis_index("x")
    kv = lax.axis_index("y") // 2
    key_own = lax.dynamic_slice_in_dim(keys, kv * HEAD_DIM, HEAD_DIM, 1)
    value_own = lax.dynamic_slice_in_dim(values, kv * HEAD_DIM, HEAD_DIM, 1)

    pack = jnp.concatenate([key_own, value_own, target], axis=0)
    half = pack.shape[0] // 2
    from_left = shifted(pack, "x", 1)
    from_right = shifted(pack, "x", -1)
    far_low = shifted(from_left[:half], "x", 1)
    far_high = shifted(from_right[half:], "x", -1)
    far = jnp.concatenate([far_low, far_high], axis=0)
    blocks = [pack, from_left, from_right, far]
    key_all = jnp.concatenate([b[:src] for b in blocks], axis=0)
    value_all = jnp.concatenate([b[src : 2 * src] for b in blocks], axis=0)

    both = told_all(jnp.concatenate([queries, grad_out], axis=1), "z")
    both = both.reshape(nz * rows, 2 * cols)
    query_all, grad_all = both[:, :cols], both[:, cols:]
    n_rows = nz * rows

    delta_own = jnp.sum(attn_out.astype(F32) * grad_out.astype(F32), axis=1)
    scores = dot(key_all, query_all, 1, 1) * SCALE
    peak = jnp.max(scores, axis=0)
    total = jnp.sum(jnp.exp(scores - peak[None]), axis=0)
    stats = jnp.concatenate([peak, total, delta_own]).reshape(-1, 128)
    stats = told_all(jnp.pad(stats, ((0, 24 - stats.shape[0]), (0, 0))), "z").reshape(nz, 24, 128)
    peaks = stats[:, :8].reshape(nz, n_rows)
    totals = stats[:, 8:16].reshape(nz, n_rows)
    deltas = stats[:, 16].reshape(n_rows)
    top = jnp.max(peaks, axis=0)
    log_totals = top + jnp.log(jnp.sum(totals * jnp.exp(peaks - top[None]), axis=0))

    weights = jnp.exp(scores - log_totals[None])
    grad_weights = dot(value_all, grad_all, 1, 1)
    grad_scores = (weights * (grad_weights - deltas[None]) * SCALE).astype(BF16)
    key_sum = dot(grad_scores, query_all, 1, 0)
    value_sum = dot(weights.astype(BF16), grad_all, 1, 0)
    query_t = dot(key_all, grad_scores, 0, 0)

    sent = query_t.astype(BF16).reshape(nx, cols // nx, nz, rows).transpose(2, 0, 1, 3)
    got = exchanged(sent.reshape(nz * nx, cols // nx, rows), ("z", "x"))
    got = got.reshape(nz, nx, cols // nx, rows).astype(F32).sum(axis=0)
    part_t = got.transpose(1, 0, 2).reshape(cols // nx, nx * rows).astype(BF16)

    offsets = (0, -1, 1, 2)
    target_t = jnp.zeros((cols, nx * rows), BF16)
    for b, off in zip(blocks, offsets):
        at = lax.rem(x_at + off + nx, nx) * rows
        target_t = lax.dynamic_update_slice(target_t, b[2 * src :].T, (0, at))
    wide_t = target_t.astype(F32)
    squares = jnp.sum(wide_t * wide_t, axis=0)
    high = squares.astype(BF16)
    low = (squares - high.astype(F32)).astype(BF16)
    extra = jnp.concatenate([high[None], low[None], jnp.zeros((6, nx * rows), BF16)], axis=0)
    piece = jnp.concatenate([part_t, extra], axis=0)
    column = told_all(piece, "y")
    other = shifted(column, "c", 1)
    first = jnp.where(core == 0, column, other).reshape(8, 1, 72, nx * rows)
    second = jnp.where(core == 0, other, column).reshape(8, 1, 72, nx * rows)
    every = jnp.concatenate([first, second], axis=1).reshape(HEADS, 72, nx * rows)
    grad_t = every[:, :64].reshape(HEADS * 64, nx * rows)
    squares_all = every[:, 64:66].astype(F32).sum(axis=(0, 1))
    inverse = lax.rsqrt(squares_all / WIDTH + EPS)
    normed_t = (wide_t * inverse[None] * gain[:, None]).astype(BF16)

    w_own = lax.dynamic_slice(
        w_query.reshape(cols, HEADS, nx, 64), (0, 0, x_at, 0), (cols, HEADS, 1, 64)
    ).reshape(cols, HEADS * 64)
    rows_t = dot(w_own, grad_t, 1, 0).astype(BF16)
    weight_part = dot(normed_t, grad_t, 1, 1).astype(BF16)

    rows_sent = rows_t.reshape(cols, nx, rows).transpose(1, 0, 2)
    grad_rows = exchanged(rows_sent, "x").astype(F32).sum(axis=0).T.astype(BF16)

    weight_got = exchanged(weight_part.reshape(nz * nx, 8, HEADS * 64), ("z", "x"))
    weight_got = weight_got.reshape(nz, nx, 8, HEADS, 64).astype(F32).sum(axis=0)
    grad_weight = weight_got.transpose(1, 2, 0, 3).reshape(8, WIDTH)

    mine = jnp.where(core == 0, key_sum, value_sum)
    theirs = jnp.where(core == 0, value_sum, key_sum).astype(BF16)
    mine = mine + shifted(theirs, "c", 1).astype(F32)
    own, left, right, away = (mine[src * k : src * (k + 1)] for k in range(4))
    h = src // 2
    low_in = shifted(away[:h].astype(BF16), "x", 1)
    high_in = shifted(away[h:].astype(BF16), "x", -1)
    right = jnp.concatenate([right[:h] + low_in.astype(F32), right[h:]], axis=0)
    left = jnp.concatenate([left[:h], left[h:] + high_in.astype(F32)], axis=0)
    got_r = shifted(right.astype(BF16), "x", 1)
    got_l = shifted(left.astype(BF16), "x", -1)
    own = (own + got_r.astype(F32) + got_l.astype(F32)).astype(BF16)
    parts = exchanged(own.reshape(HEADS, src // HEADS, HEAD_DIM), ("y", "c"))
    parts = parts.reshape(KV_HEADS, 2, 2, src // HEADS, HEAD_DIM).astype(F32).sum(axis=1)
    parts = parts.transpose(1, 2, 0, 3).reshape(2, src // HEADS, KV_HEADS * HEAD_DIM)
    return (grad_rows, grad_weight, parts[0], parts[1])


def solution(mesh):
    finer = Mesh(mesh.devices.reshape(8, 4, 8, 2), ("z", "x", "y", "c"))
    sp, tp = ("z", "x"), ("y", "c")
    placed = (
        P(sp, tp),
        P(tp),
        P(tp, None),
        P(sp, tp),
        P(sp, None),
        P(sp, None),
        P(sp, tp),
        P(sp, tp),
    )
    return jax.shard_map(
        local,
        mesh=finer,
        in_specs=placed,
        out_specs=(P(sp, tp), P(tp + sp, None), P(sp + tp, None), P(sp + tp, None)),
        check_vma=False,
    )
```

```python
import jax
import jax.numpy as jnp
from jax import lax
from jax.sharding import Mesh
from jax.sharding import PartitionSpec as P

WIDTH = 4096
HEADS = 16
KV_HEADS = 4
HEAD_DIM = 256
EPS = 1e-06
SCALE = HEAD_DIM ** (-0.5)
F32 = jnp.float32
BF16 = jnp.bfloat16


def shifted(value, axis, by):
    n = lax.axis_size(axis)
    return lax.ppermute(value, axis, [(i, (i + by) % n) for i in range(n)])


def exchanged(value, axis):
    return lax.all_to_all(value, axis, split_axis=0, concat_axis=0, tiled=True)


def told_all(value, axis):
    n = lax.axis_size(axis)
    return exchanged(jnp.broadcast_to(value[None], (n, *value.shape)), axis)


def dot(a, b, ca, cb):
    return lax.dot_general(a, b, (((ca,), (cb,)), ((), ())), preferred_element_type=F32)


def terms(value):
    high = lax.reduce_precision(value, 8, 7)
    rest = value - high
    mid = lax.reduce_precision(rest, 8, 7)
    return [t.astype(BF16) for t in (high, mid, rest - mid)]


def local(target, gain, w_query, queries, keys, values, attn_out, grad_out):
    nz, nx = lax.axis_size("z"), lax.axis_size("x")
    rows, cols = queries.shape
    part = cols // nx
    src = keys.shape[0]
    core = lax.axis_index("c")
    x_at = lax.axis_index("x")
    kv = lax.axis_index("y") // 2
    key_own = lax.dynamic_slice_in_dim(keys, kv * HEAD_DIM, HEAD_DIM, 1)
    value_own = lax.dynamic_slice_in_dim(values, kv * HEAD_DIM, HEAD_DIM, 1)

    pack = jnp.concatenate([key_own, value_own, target], axis=0)
    half = pack.shape[0] // 2
    from_left = shifted(pack, "x", 1)
    from_right = shifted(pack, "x", -1)
    far_low = shifted(from_left[:half], "x", 1)
    far_high = shifted(from_right[half:], "x", -1)
    far = jnp.concatenate([far_low, far_high], axis=0)
    blocks = ((pack, 0), (from_left, 3), (from_right, 1), (far, 2))

    def assembled(first, last):
        out = jnp.zeros((nx * (last - first), cols), BF16)
        for block, off in blocks:
            at = lax.rem(x_at + off, nx) * (last - first)
            out = lax.dynamic_update_slice(out, block[first:last], (at, 0))
        return out

    key_all = assembled(0, src)
    value_all = assembled(src, 2 * src)
    target_all = assembled(2 * src, 2 * src + rows)

    delta_own = jnp.sum(attn_out.astype(F32) * grad_out.astype(F32), axis=1)
    line = jnp.concatenate(terms(delta_own) + [jnp.zeros((rows,), BF16)])[None]
    both = jnp.concatenate([queries, grad_out], axis=1)
    both = jnp.concatenate([both, line, jnp.zeros((7, 2 * cols), BF16)], axis=0)
    both = told_all(both, "z").reshape(nz, rows + 8, 2 * cols)
    query_all = both[:, :rows, :cols].reshape(nz * rows, cols)
    grad_all = both[:, :rows, cols:].reshape(nz * rows, cols)
    deltas = both[:, rows].astype(F32).reshape(nz, 4, rows).sum(axis=1).reshape(nz * rows)

    w_parts = lax.dynamic_slice(
        w_query.reshape(cols, HEADS // 2, 2, nx, part), (0, 0, 0, x_at, 0), (cols, HEADS // 2, 2, 1, part)
    )
    w_even = w_parts[:, :, 0].reshape(cols, -1)
    w_odd = w_parts[:, :, 1].reshape(cols, -1)
    w_mine = jnp.where(core == 0, w_even, w_odd)
    w_theirs = jnp.where(core == 0, w_odd, w_even)
    target_t = lax.optimization_barrier(target_all).T
    swapped = shifted(jnp.concatenate([target_t, w_theirs], axis=1), "c", 1)
    other_t, w_other = swapped[:, : nx * rows], swapped[:, nx * rows :]

    def by_core(mine, theirs):
        return jnp.where(core == 0, jnp.stack([mine, theirs]), jnp.stack([theirs, mine]))

    target_both = by_core(target_t, other_t).astype(F32)
    w_both = by_core(w_mine, w_other).reshape(2 * cols, -1)
    squares = jnp.sum(target_both * target_both, axis=(0, 1))

    scores = dot(key_all, query_all, 1, 1) * SCALE
    peak = jnp.max(scores, axis=0)
    weights = jnp.exp(scores - peak[None])
    total = jnp.sum(weights, axis=0)
    stats = told_all(jnp.concatenate([peak, total]).reshape(2 * nz, rows), "z").reshape(nz, 2, nz * rows)
    grad_weights = dot(value_all, grad_all, 1, 1)
    grad_scores = (weights * ((grad_weights - deltas[None]) * SCALE)).astype(BF16)
    query_t = dot(key_all, grad_scores, 0, 0)
    query_t, stats = lax.optimization_barrier((query_t, stats))
    top = jnp.max(stats[:, 0], axis=0)
    log_totals = top + jnp.log(jnp.sum(stats[:, 1] * jnp.exp(stats[:, 0] - top[None]), axis=0))
    share = jnp.exp(peak - log_totals)

    sent = (query_t * share[None]).astype(BF16).reshape(nx, part, nz, rows).transpose(2, 0, 1, 3)
    got = exchanged(sent.reshape(nz * nx, part, rows), ("z", "x")).reshape(nz, nx, part, rows)
    part_t = got.astype(F32).sum(axis=0)
    part_t = part_t.transpose(1, 0, 2).reshape(part, nx * rows).astype(BF16)

    key_sum = dot(grad_scores, (query_all * share[:, None]).astype(BF16), 1, 0)
    value_sum = dot(weights.astype(BF16), (grad_all * share[:, None]).astype(BF16), 1, 0)
    key_sum = key_sum.reshape(nx, src, HEAD_DIM)
    value_sum = value_sum.reshape(nx, src, HEAD_DIM)

    def block_at(off):
        at = lax.rem(x_at + off, nx)
        return [lax.dynamic_index_in_dim(v, at, 0, keepdims=False) for v in (key_sum, value_sum)]

    own_k, own_v = block_at(0)
    right_k, right_v = block_at(1)
    far_k, far_v = block_at(2)
    left_k, left_v = block_at(3)
    low_in = shifted(far_k.astype(BF16), "x", 1)
    high_in = shifted(far_v.astype(BF16), "x", -1)
    right = jnp.concatenate([right_k + low_in.astype(F32), right_v], axis=0).astype(BF16)
    left = jnp.concatenate([left_k, left_v + high_in.astype(F32)], axis=0).astype(BF16)
    arrived = shifted(right, "x", 1).astype(F32) + shifted(left, "x", -1).astype(F32)
    own_k = own_k + arrived[:src]
    own_v = own_v + arrived[src:]
    mine = jnp.where(core == 0, own_k, own_v)
    theirs = jnp.where(core == 0, own_v, own_k).astype(BF16)
    mine = (mine + shifted(theirs, "c", 1).astype(F32)).astype(BF16)

    high = lax.reduce_precision(squares, 8, 7)
    extra = jnp.stack([high, squares - high]).astype(BF16)
    piece = jnp.concatenate([part_t, extra, jnp.zeros((6, nx * rows), BF16)], axis=0)
    every = told_all(piece, "y").reshape(HEADS // 2, part + 8, nx * rows)
    grad_t = every[:, :part].reshape(HEADS // 2 * part, nx * rows)
    squares_all = every[:, part : part + 2].astype(F32).sum(axis=(0, 1))
    inverse = lax.rsqrt(squares_all / WIDTH + EPS)
    normed_t = (target_both * inverse[None, None]).astype(BF16)
    weight_part = dot(normed_t.reshape(2 * cols, -1), grad_t, 1, 1).astype(BF16)

    weight_sent = weight_part.reshape(2, nz * nx, 8, -1).transpose(1, 0, 2, 3).reshape(nz * nx * 2, 8, -1)
    weight_got = exchanged(weight_sent, ("z", "x", "c"))
    weight_sum = weight_got.reshape(nz, nx * 2, 8, HEADS // 2 * part).astype(F32).sum(axis=0)
    gain_at = (lax.axis_index("z") * nx + x_at) * 8
    weight_sum = weight_sum * lax.dynamic_slice_in_dim(gain, gain_at, 8, 0)[None, :, None]
    weight_sum = lax.optimization_barrier(weight_sum).reshape(nx, 2, 8, HEADS // 2, part)
    grad_weight = weight_sum.transpose(2, 3, 1, 0, 4).reshape(8, WIDTH)

    grad_t, _ = lax.optimization_barrier((grad_t, weight_sent))
    rows_t = dot(w_both, grad_t, 1, 0)

    def rows_at(off):
        return lax.dynamic_slice_in_dim(rows_t, lax.rem(x_at + off, nx) * rows, rows, 1)

    rows_sum = rows_at(0)
    for off, by in ((1, 1), (3, -1), (2, 2)):
        rows_sum = rows_sum + shifted(rows_at(off).astype(BF16), "x", by).astype(F32)
    low, high = rows_sum[:cols], rows_sum[cols:]
    rows_in = shifted(jnp.where(core == 0, high, low).astype(BF16), "c", 1)
    grad_rows = (jnp.where(core == 0, low, high) + rows_in.astype(F32)).T.astype(BF16)

    mine, _ = lax.optimization_barrier((mine, weight_got))
    sums = exchanged(mine.reshape(HEADS, src // HEADS, HEAD_DIM), ("y", "c"))
    sums = sums.reshape(KV_HEADS, 2, 2, src // HEADS, HEAD_DIM).astype(F32).sum(axis=1)
    sums = sums.transpose(1, 2, 0, 3).reshape(2, src // HEADS, -1)
    return (grad_rows, grad_weight, sums[0], sums[1])


def solution(mesh):
    finer = Mesh(mesh.devices.reshape(8, 4, 8, 2), ("z", "x", "y", "c"))
    sp, tp = ("z", "x"), ("y", "c")
    placed = (
        P(sp, tp),
        P(tp),
        P(tp, None),
        P(sp, tp),
        P(sp, None),
        P(sp, None),
        P(sp, tp),
        P(sp, tp),
    )
    return jax.shard_map(
        local,
        mesh=finer,
        in_specs=placed,
        out_specs=(P(sp, tp), P(tp + sp, None), P(sp + tp, None), P(sp + tp, None)),
        check_vma=False,
    )
```

```python
import jax
import jax.numpy as jnp
from jax import lax
from jax.experimental.layout import Layout, with_layout_constraint
from jax.sharding import Mesh
from jax.sharding import PartitionSpec as P

WIDTH = 4096
HEADS = 16
KV_HEADS = 4
HEAD_DIM = 256
EPS = 1e-06
SCALE = HEAD_DIM ** (-0.5)
F32 = jnp.float32
BF16 = jnp.bfloat16


def shifted(value, axis, by):
    n = lax.axis_size(axis)
    return lax.ppermute(value, axis, [(i, (i + by) % n) for i in range(n)])


def exchanged(value, axis):
    return lax.all_to_all(value, axis, split_axis=0, concat_axis=0, tiled=True)


def told_all(value, axis):
    n = lax.axis_size(axis)
    return exchanged(jnp.broadcast_to(value[None], (n, *value.shape)), axis)


def dot(a, b, ca, cb):
    return lax.dot_general(a, b, (((ca,), (cb,)), ((), ())), preferred_element_type=F32)


def row_major(value):
    return with_layout_constraint(value, Layout(major_to_minor=tuple(range(value.ndim))))


def terms(value):
    high = lax.reduce_precision(value, 8, 7)
    rest = value - high
    mid = lax.reduce_precision(rest, 8, 7)
    return [t.astype(BF16) for t in (high, mid, rest - mid)]


def local(target, gain, w_query, queries, keys, values, attn_out, grad_out):
    nz, nx = lax.axis_size("z"), lax.axis_size("x")
    rows, cols = queries.shape
    part = cols // nx
    src = keys.shape[0]
    core = lax.axis_index("c")
    x_at = lax.axis_index("x")
    kv = lax.axis_index("y") // 2
    key_own = lax.dynamic_slice_in_dim(keys, kv * HEAD_DIM, HEAD_DIM, 1)
    value_own = lax.dynamic_slice_in_dim(values, kv * HEAD_DIM, HEAD_DIM, 1)

    query_all = told_all(queries, "z").reshape(nz * rows, cols)
    pack = row_major(jnp.concatenate([key_own, value_own, target], axis=0))
    half = pack.shape[0] // 2
    from_left = shifted(pack, "x", 1)
    from_right = shifted(pack, "x", -1)
    from_left, from_right, query_all = lax.optimization_barrier((from_left, from_right, query_all))
    far_low = shifted(from_left[:half], "x", 1)
    far_high = shifted(from_right[half:], "x", -1)
    far = jnp.concatenate([far_low, far_high], axis=0)
    blocks = ((pack, 0), (from_left, 3), (from_right, 1), (far, 2))

    def assembled(first, last):
        out = jnp.zeros((nx * (last - first), cols), BF16)
        for block, off in blocks:
            at = lax.rem(x_at + off, nx) * (last - first)
            out = lax.dynamic_update_slice(out, block[first:last], (at, 0))
        return out

    key_all = row_major(assembled(0, src))
    value_all = row_major(assembled(src, 2 * src))
    target_all = assembled(2 * src, 2 * src + rows)

    delta_own = jnp.sum(attn_out.astype(F32) * grad_out.astype(F32), axis=1)
    line = jnp.concatenate(terms(delta_own) + [jnp.zeros((5 * rows,), BF16)]).reshape(4, cols)
    both = row_major(jnp.concatenate([grad_out, line, jnp.zeros((4, cols), BF16)], axis=0))
    both = told_all(both, "z").reshape(nz, rows + 8, cols)

    scores = dot(key_all, query_all, 1, 1) * SCALE
    peak = jnp.max(scores, axis=0)
    weights = jnp.exp(scores - peak[None])
    total = jnp.sum(weights, axis=0)
    stats = told_all(jnp.concatenate([peak, total]).reshape(2 * nz, rows), "z").reshape(nz, 2, nz * rows)
    both, total = lax.optimization_barrier((both, total))
    grad_all = both[:, :rows].reshape(nz * rows, cols)
    deltas = both[:, rows : rows + 2].astype(F32).reshape(nz, 4, rows)[:, :3].sum(axis=1).reshape(nz * rows)
    grad_weights = dot(value_all, grad_all, 1, 1)
    grad_scores = (weights * ((grad_weights - deltas[None]) * SCALE)).astype(BF16)
    query_t = dot(key_all, grad_scores, 0, 0)
    query_t, stats = lax.optimization_barrier((query_t, stats))
    top = jnp.max(stats[:, 0], axis=0)
    log_totals = top + jnp.log(jnp.sum(stats[:, 1] * jnp.exp(stats[:, 0] - top[None]), axis=0))
    share = jnp.exp(peak - log_totals)

    sent = (query_t * share[None]).astype(BF16).reshape(nx, part, nz, rows).transpose(2, 0, 1, 3)
    sent = sent.reshape(nz * nx, part, rows)
    got = exchanged(sent, ("z", "x")).reshape(nz, nx, part, rows)
    part_t = got.astype(F32).sum(axis=0)
    part_t = part_t.transpose(1, 0, 2).reshape(part, nx * rows).astype(BF16)

    key_sum = dot(grad_scores, (query_all * share[:, None]).astype(BF16), 1, 0)
    value_sum = dot(weights.astype(BF16), (grad_all * share[:, None]).astype(BF16), 1, 0)
    mine = jnp.where(core == 0, key_sum, value_sum)
    theirs = jnp.where(core == 0, value_sum, key_sum).astype(BF16)
    mine = (mine + shifted(theirs, "c", 1).astype(F32)).astype(BF16).reshape(nx, src, HEAD_DIM)

    def block_at(off):
        return lax.dynamic_index_in_dim(mine, lax.rem(x_at + off, nx), 0, keepdims=False)

    own = block_at(0).astype(F32)
    for off, by in ((2, 2), (1, 1), (3, -1)):
        own = own + shifted(block_at(off), "x", by).astype(F32)
    mine = own.astype(BF16)

    w_parts = lax.dynamic_slice(
        w_query.reshape(cols, HEADS // 2, 2, nx, part), (0, 0, 0, x_at, 0), (cols, HEADS // 2, 2, 1, part)
    )
    w_even = w_parts[:, :, 0].reshape(cols, -1)
    w_odd = w_parts[:, :, 1].reshape(cols, -1)
    w_mine = jnp.where(core == 0, w_even, w_odd)
    w_theirs = jnp.where(core == 0, w_odd, w_even)
    target_all, w_theirs, _ = lax.optimization_barrier((target_all, w_theirs, sent))
    target_t = target_all.T
    swapped = shifted(jnp.concatenate([target_t, w_theirs], axis=1), "c", 1)
    other_t, w_other = swapped[:, : nx * rows], swapped[:, nx * rows :]

    def by_core(mine, theirs):
        return jnp.where(core == 0, jnp.stack([mine, theirs]), jnp.stack([theirs, mine]))

    target_both = by_core(target_t, other_t).astype(F32)
    w_both = by_core(w_mine, w_other).reshape(2 * cols, -1)
    squares = jnp.sum(target_both * target_both, axis=(0, 1))

    high = lax.reduce_precision(squares, 8, 7)
    extra = jnp.stack([high, squares - high]).astype(BF16)
    piece = jnp.concatenate([part_t, extra, jnp.zeros((6, nx * rows), BF16)], axis=0)
    every = told_all(piece, "y").reshape(HEADS // 2, part + 8, nx * rows)
    every, mine = lax.optimization_barrier((every, mine))
    grad_t = every[:, :part].reshape(HEADS // 2 * part, nx * rows)
    squares_all = every[:, part : part + 2].astype(F32).sum(axis=(0, 1))
    inverse = lax.rsqrt(squares_all / WIDTH + EPS)
    normed_t = (target_both * inverse[None, None]).astype(BF16)
    weight_part = dot(normed_t.reshape(2 * cols, -1), grad_t, 1, 1).astype(BF16)

    weight_sent = weight_part.reshape(2, nz * nx, 8, -1).transpose(1, 0, 2, 3).reshape(nz * nx * 2, 8, -1)
    weight_got = exchanged(weight_sent, ("z", "x", "c"))
    weight_sum = weight_got.reshape(nz, nx * 2, 8, HEADS // 2 * part).astype(F32).sum(axis=0)
    gain_at = (lax.axis_index("z") * nx + x_at) * 8
    weight_sum = weight_sum * lax.dynamic_slice_in_dim(gain, gain_at, 8, 0)[None, :, None]
    weight_sum = lax.optimization_barrier(weight_sum).reshape(nx, 2, 8, HEADS // 2, part)
    grad_weight = weight_sum.transpose(2, 3, 1, 0, 4).reshape(8, WIDTH)

    grad_t, _ = lax.optimization_barrier((grad_t, weight_sent))
    rows_t = dot(w_both, grad_t, 1, 0)

    def rows_at(off):
        return lax.dynamic_slice_in_dim(rows_t, lax.rem(x_at + off, nx) * rows, rows, 1)

    rows_sum = rows_at(0)
    for off, by in ((1, 1), (3, -1), (2, 2)):
        rows_sum = rows_sum + shifted(rows_at(off).astype(BF16), "x", by).astype(F32)
    low, high = rows_sum[:cols], rows_sum[cols:]
    rows_in = shifted(jnp.where(core == 0, high, low).astype(BF16), "c", 1)
    grad_rows = (jnp.where(core == 0, low, high) + rows_in.astype(F32)).T.astype(BF16)

    mine, _ = lax.optimization_barrier((mine, weight_got))
    sums = exchanged(mine.reshape(HEADS, src // HEADS, HEAD_DIM), ("y", "c"))
    sums = sums.reshape(KV_HEADS, 2, 2, src // HEADS, HEAD_DIM).astype(F32).sum(axis=1)
    sums = sums.transpose(1, 2, 0, 3).reshape(2, src // HEADS, -1)
    return (grad_rows, grad_weight, sums[0], sums[1])


def solution(mesh):
    finer = Mesh(mesh.devices.reshape(8, 4, 8, 2), ("z", "x", "y", "c"))
    sp, tp = ("z", "x"), ("y", "c")
    placed = (
        P(sp, tp),
        P(tp),
        P(tp, None),
        P(sp, tp),
        P(sp, None),
        P(sp, None),
        P(sp, tp),
        P(sp, tp),
    )
    return jax.shard_map(
        local,
        mesh=finer,
        in_specs=placed,
        out_specs=(P(sp, tp), P(tp + sp, None), P(sp + tp, None), P(sp + tp, None)),
        check_vma=False,
    )
```

```python
import jax
import jax.numpy as jnp
from jax import lax
from jax.experimental.layout import Layout, with_layout_constraint
from jax.sharding import Mesh
from jax.sharding import PartitionSpec as P

WIDTH = 4096
HEADS = 16
KV_HEADS = 4
HEAD_DIM = 256
EPS = 1e-06
SCALE = HEAD_DIM ** (-0.5)
F32 = jnp.float32
BF16 = jnp.bfloat16


def shifted(value, axis, by):
    n = lax.axis_size(axis)
    return lax.ppermute(value, axis, [(i, (i + by) % n) for i in range(n)])


def exchanged(value, axis):
    return lax.all_to_all(value, axis, split_axis=0, concat_axis=0, tiled=True)


def told_all(value, axis):
    n = lax.axis_size(axis)
    return exchanged(jnp.broadcast_to(value[None], (n, *value.shape)), axis)


def dot(a, b, ca, cb):
    return lax.dot_general(a, b, (((ca,), (cb,)), ((), ())), preferred_element_type=F32)


def row_major(value):
    return with_layout_constraint(value, Layout(major_to_minor=tuple(range(value.ndim))))


def terms(value):
    high = lax.reduce_precision(value, 8, 7)
    rest = value - high
    mid = lax.reduce_precision(rest, 8, 7)
    return [t.astype(BF16) for t in (high, mid, rest - mid)]


def local(target, gain, w_query, queries, keys, values, attn_out, grad_out):
    nz, nx, ny = lax.axis_size("z"), lax.axis_size("x"), lax.axis_size("y")
    rows, cols = queries.shape
    part = cols // nx
    src = keys.shape[0]
    bit = src // (2 * ny)
    core = lax.axis_index("c")
    x_at = lax.axis_index("x")
    kv = lax.axis_index("y") // 2
    n_rows = nz * rows

    delta_own = jnp.sum(attn_out.astype(F32) * grad_out.astype(F32), axis=1)
    line = jnp.concatenate(terms(delta_own) + [jnp.zeros((rows,), BF16)])[None]
    both = jnp.concatenate([queries, grad_out], axis=1)
    both = jnp.concatenate([both, line, jnp.zeros((7, 2 * cols), BF16)], axis=0)
    both = told_all(both, "z")

    def half_of(v):
        v = v.reshape(ny, 2, bit, v.shape[1])
        v = lax.dynamic_slice(v, (0, core, 0, kv * HEAD_DIM), (ny, 1, bit, HEAD_DIM))
        return v.reshape(src // 2, HEAD_DIM)

    pack = row_major(jnp.concatenate([half_of(keys), half_of(values), target], axis=0))
    blocks = [pack] + [shifted(pack, "x", by) for by in (1, -1, 2)]
    target_all = jnp.zeros((nx * rows, cols), BF16)
    for block, off in zip(blocks, (0, 3, 1, 2)):
        target_all = lax.dynamic_update_slice(target_all, block[src:], (lax.rem(x_at + off, nx) * rows, 0))

    w_parts = lax.dynamic_slice(
        w_query.reshape(cols, HEADS // 2, 2, nx, part), (0, 0, 0, x_at, 0), (cols, HEADS // 2, 2, 1, part)
    )
    w_even = w_parts[:, :, 0].reshape(cols, -1)
    w_odd = w_parts[:, :, 1].reshape(cols, -1)
    w_mine = jnp.where(core == 0, w_even, w_odd)
    w_theirs = jnp.where(core == 0, w_odd, w_even)
    swap = [b[:src] for b in blocks] + [target_all, w_theirs[:, :cols], w_theirs[:, cols:]]
    swap = shifted(row_major(jnp.concatenate(swap, axis=0)), "c", 1)
    blocks = [b[:src] for b in blocks] + [swap[src * k : src * (k + 1)] for k in range(nx)]
    key_all = row_major(jnp.concatenate([b[: src // 2] for b in blocks], axis=0))
    value_all = row_major(jnp.concatenate([b[src // 2 :] for b in blocks], axis=0))
    target_other = swap[nx * src : nx * src + nx * rows]
    w_other = swap[nx * src + nx * rows :]
    w_other = jnp.concatenate([w_other[:cols], w_other[cols:]], axis=1)

    both = both.reshape(nz, rows + 8, 2 * cols)
    query_all = both[:, :rows, :cols].reshape(n_rows, cols)
    grad_all = both[:, :rows, cols:].reshape(n_rows, cols)
    deltas = both[:, rows].astype(F32).reshape(nz, 4, rows).sum(axis=1).reshape(n_rows)
    scores = dot(key_all, query_all, 1, 1) * SCALE
    peak = jnp.max(scores, axis=0)
    weights = jnp.exp(scores - peak[None])
    total = jnp.sum(weights, axis=0)
    stats = told_all(jnp.concatenate([peak, total]).reshape(2 * nz, rows), "z").reshape(nz, 2, n_rows)
    grad_weights = dot(value_all, grad_all, 1, 1)
    grad_scores = (weights * ((grad_weights - deltas[None]) * SCALE)).astype(BF16)
    query_t = dot(key_all, grad_scores, 0, 0)
    query_t, stats = lax.optimization_barrier((query_t, stats))
    top = jnp.max(stats[:, 0], axis=0)
    log_totals = top + jnp.log(jnp.sum(stats[:, 1] * jnp.exp(stats[:, 0] - top[None]), axis=0))
    share = jnp.exp(peak - log_totals)

    sent = (query_t * share[None]).astype(BF16).reshape(nx, part, nz, rows).transpose(2, 0, 1, 3)
    sent = sent.reshape(nz * nx, part, rows)
    got = exchanged(sent, ("z", "x")).reshape(nz, nx, part, rows)
    part_t = got.astype(F32).sum(axis=0)
    part_t = part_t.transpose(1, 0, 2).reshape(part, nx * rows).astype(BF16)

    query_share, grad_share, _ = lax.optimization_barrier(
        ((query_all * share[:, None]).astype(BF16), (grad_all * share[:, None]).astype(BF16), sent)
    )
    key_sum = dot(grad_scores, query_share, 1, 0)
    value_sum = dot(weights.astype(BF16), grad_share, 1, 0)
    half = nx * src // 2
    theirs = jnp.concatenate([key_sum[half:], value_sum[half:]], axis=1).astype(BF16)
    mine = jnp.concatenate([key_sum[:half], value_sum[:half]], axis=1)
    mine = row_major((mine + shifted(row_major(theirs), "c", 1).astype(F32)).astype(BF16))
    own, left, right, far = (mine[src // 2 * k : src // 2 * (k + 1)] for k in range(nx))
    own = own.astype(F32)
    for block, by in ((far, 2), (right, 1), (left, -1)):
        own = own + shifted(block, "x", by).astype(F32)
    mine = own.astype(BF16)

    def by_core(mine, theirs):
        return jnp.where(core == 0, jnp.stack([mine, theirs]), jnp.stack([theirs, mine]))

    target_both = by_core(target_all.T, target_other.T).astype(F32)
    w_both = by_core(w_mine, w_other).reshape(2 * cols, -1)
    squares = jnp.sum(target_both * target_both, axis=(0, 1))
    high = lax.reduce_precision(squares, 8, 7)
    extra = jnp.stack([high, squares - high]).astype(BF16)
    piece = jnp.concatenate([part_t, extra, jnp.zeros((6, nx * rows), BF16)], axis=0)
    every = told_all(piece, "y").reshape(HEADS // 2, part + 8, nx * rows)
    every, mine = lax.optimization_barrier((every, mine))
    grad_t = every[:, :part].reshape(HEADS // 2 * part, nx * rows)
    squares_all = every[:, part : part + 2].astype(F32).sum(axis=(0, 1))
    inverse = lax.rsqrt(squares_all / WIDTH + EPS)
    normed_t = (target_both * inverse[None, None]).astype(BF16)
    weight_part = dot(normed_t.reshape(2 * cols, -1), grad_t, 1, 1).astype(BF16)

    weight_sent = weight_part.reshape(2, nz * nx, 8, -1).transpose(1, 0, 2, 3).reshape(nz * nx * 2, 8, -1)
    weight_got = exchanged(weight_sent, ("z", "x", "c"))
    weight_sum = weight_got.reshape(nz, nx * 2, 8, HEADS // 2 * part).astype(F32).sum(axis=0)
    gain_at = (lax.axis_index("z") * nx + x_at) * 8
    weight_sum = weight_sum * lax.dynamic_slice_in_dim(gain, gain_at, 8, 0)[None, :, None]
    weight_sum = lax.optimization_barrier(weight_sum).reshape(nx, 2, 8, HEADS // 2, part)
    grad_weight = weight_sum.transpose(2, 3, 1, 0, 4).reshape(8, WIDTH)

    grad_t, _ = lax.optimization_barrier((grad_t, weight_sent))
    rows_t = dot(w_both, grad_t, 1, 0)

    def rows_at(off):
        return lax.dynamic_slice_in_dim(rows_t, lax.rem(x_at + off, nx) * rows, rows, 1)

    rows_sum = rows_at(0)
    for off, by in ((1, 1), (3, -1), (2, 2)):
        rows_sum = rows_sum + shifted(rows_at(off).astype(BF16), "x", by).astype(F32)
    low, high = rows_sum[:cols], rows_sum[cols:]
    rows_in = shifted(jnp.where(core == 0, high, low).astype(BF16), "c", 1)
    grad_rows = (jnp.where(core == 0, low, high) + rows_in.astype(F32)).T.astype(BF16)

    mine, _ = lax.optimization_barrier((mine, weight_got))
    sums = exchanged(mine.reshape(ny, bit, 2 * HEAD_DIM), "y")
    sums = sums.reshape(KV_HEADS, 2, bit, 2, HEAD_DIM).astype(F32).sum(axis=1)
    sums = sums.transpose(2, 1, 0, 3).reshape(2, bit, KV_HEADS * HEAD_DIM)
    return (grad_rows, grad_weight, sums[0], sums[1])


def solution(mesh):
    finer = Mesh(mesh.devices.reshape(8, 4, 8, 2), ("z", "x", "y", "c"))
    sp, tp = ("z", "x"), ("y", "c")
    placed = (
        P(sp, tp),
        P(tp),
        P(tp, None),
        P(sp, tp),
        P(sp, None),
        P(sp, None),
        P(sp, tp),
        P(sp, tp),
    )

    return jax.shard_map(
        local,
        mesh=finer,
        in_specs=placed,
        out_specs=(P(sp, tp), P(tp + sp, None), P(sp + tp, None), P(sp + tp, None)),
        check_vma=False,
    )
```

```python
import jax
import jax.numpy as jnp
from jax import lax
from jax.experimental.layout import Layout, with_layout_constraint
from jax.sharding import Mesh
from jax.sharding import PartitionSpec as P

WIDTH = 4096
HEADS = 16
KV_HEADS = 4
HEAD_DIM = 256
EPS = 1e-06
SCALE = HEAD_DIM ** (-0.5)
F32 = jnp.float32
BF16 = jnp.bfloat16


def shifted(value, axis, by):
    n = lax.axis_size(axis)
    return lax.ppermute(value, axis, [(i, (i + by) % n) for i in range(n)])


def exchanged(value, axis):
    return lax.all_to_all(value, axis, split_axis=0, concat_axis=0, tiled=True)


def told_all(value, axis):
    n = lax.axis_size(axis)
    return exchanged(jnp.broadcast_to(value[None], (n, *value.shape)), axis)


def dot(a, b, ca, cb):
    return lax.dot_general(a, b, (((ca,), (cb,)), ((), ())), preferred_element_type=F32)


def row_major(value):
    return with_layout_constraint(value, Layout(major_to_minor=tuple(range(value.ndim))))


def terms(value):
    high = lax.reduce_precision(value, 8, 7)
    rest = value - high
    mid = lax.reduce_precision(rest, 8, 7)
    return [t.astype(BF16) for t in (high, mid, rest - mid)]


def local(target, gain, w_query, queries, keys, values, attn_out, grad_out):
    nz, nx, ny = lax.axis_size("z"), lax.axis_size("x"), lax.axis_size("y")
    rows, cols = queries.shape
    part = cols // nx
    src = keys.shape[0]
    bit = src // (2 * ny)
    core = lax.axis_index("c")
    x_at = lax.axis_index("x")
    kv = lax.axis_index("y") // 2
    n_rows = nz * rows

    delta_own = jnp.sum(attn_out.astype(F32) * grad_out.astype(F32), axis=1)
    line = jnp.concatenate(terms(delta_own) + [jnp.zeros((rows,), BF16)])[None]
    both = jnp.concatenate([queries, grad_out], axis=1)
    both = jnp.concatenate([both, line, jnp.zeros((7, 2 * cols), BF16)], axis=0)
    both = told_all(both, "z")

    def half_of(v):
        v = v.reshape(ny, 2, bit, v.shape[1])
        v = lax.dynamic_slice(v, (0, core, 0, kv * HEAD_DIM), (ny, 1, bit, HEAD_DIM))
        return v.reshape(src // 2, HEAD_DIM)

    halves = (target[: rows // 2], target[rows // 2 :])
    pack = jnp.concatenate([half_of(keys), half_of(values)], axis=1)
    pack = row_major(jnp.concatenate([pack, jnp.concatenate(halves, axis=1)], axis=0))
    blocks = [pack] + [row_major(shifted(pack, "x", by)) for by in (1, -1, 2)]
    half = nx * src // 2
    mine = row_major(jnp.concatenate([b[: src // 2] for b in blocks], axis=0))
    target_all = jnp.zeros((nx * rows, cols), BF16)
    for block, off in zip(blocks, (0, 3, 1, 2)):
        block = jnp.concatenate([block[src // 2 :, :cols], block[src // 2 :, cols:]], axis=0)
        target_all = lax.dynamic_update_slice(target_all, block, (lax.rem(x_at + off, nx) * rows, 0))
    target_t = row_major(row_major(target_all).T)

    w_parts = lax.dynamic_slice(
        w_query.reshape(cols, HEADS // 2, 2, nx, part), (0, 0, 0, x_at, 0), (cols, HEADS // 2, 2, 1, part)
    )
    w_even = w_parts[:, :, 0].reshape(cols, -1)
    w_odd = w_parts[:, :, 1].reshape(cols, -1)
    w_mine = jnp.where(core == 0, w_even, w_odd)
    w_theirs = jnp.where(core == 0, w_odd, w_even)
    swap = shifted(row_major(jnp.concatenate([mine, target_t, w_theirs], axis=0)), "c", 1)
    theirs, target_other, w_other = swap[:half], swap[half : half + cols], swap[half + cols :]
    key_one, value_one = mine[:, :HEAD_DIM], mine[:, HEAD_DIM:]
    key_two, value_two = theirs[:, :HEAD_DIM], theirs[:, HEAD_DIM:]

    both = both.reshape(nz, rows + 8, 2 * cols)
    query_all = both[:, :rows, :cols].reshape(n_rows, cols)
    grad_all = both[:, :rows, cols:].reshape(n_rows, cols)
    deltas = both[:, rows].astype(F32).reshape(nz, 4, rows).sum(axis=1).reshape(n_rows)
    score_one = dot(key_one, query_all, 1, 1) * SCALE
    score_two = dot(key_two, query_all, 1, 1) * SCALE
    peak = jnp.maximum(jnp.max(score_one, axis=0), jnp.max(score_two, axis=0))
    weight_one = jnp.exp(score_one - peak[None])
    weight_two = jnp.exp(score_two - peak[None])
    total = jnp.sum(weight_one, axis=0) + jnp.sum(weight_two, axis=0)
    weight_one, weight_two, total = lax.optimization_barrier(
        (weight_one.astype(BF16), weight_two.astype(BF16), total)
    )
    stats = told_all(jnp.concatenate([peak, total]).reshape(2 * nz, rows), "z").reshape(nz, 2, n_rows)

    def grads_of(weight, value):
        product = dot(value, grad_all, 1, 1)
        return (weight.astype(F32) * ((product - deltas[None]) * SCALE)).astype(BF16)

    grad_one = grads_of(weight_one, value_one)
    grad_two = grads_of(weight_two, value_two)
    query_t = dot(key_one, grad_one, 0, 0) + dot(key_two, grad_two, 0, 0)
    query_t, stats = lax.optimization_barrier((query_t, stats))
    top = jnp.max(stats[:, 0], axis=0)
    log_totals = top + jnp.log(jnp.sum(stats[:, 1] * jnp.exp(stats[:, 0] - top[None]), axis=0))
    share = jnp.exp(peak - log_totals)

    sent = (query_t * share[None]).astype(BF16).reshape(nx, part, nz, rows).transpose(2, 0, 1, 3)
    sent = sent.reshape(nz * nx, part, rows)
    got = exchanged(sent, ("z", "x")).reshape(nz, nx, part, rows)
    part_t = got.astype(F32).sum(axis=0)
    part_t = part_t.transpose(1, 0, 2).reshape(part, nx * rows).astype(BF16)

    query_share, grad_share, _ = lax.optimization_barrier(
        ((query_all * share[:, None]).astype(BF16), (grad_all * share[:, None]).astype(BF16), sent)
    )

    def sums_of(grad, weight):
        return jnp.concatenate([dot(grad, query_share, 1, 0), dot(weight, grad_share, 1, 0)], axis=1)

    swap = shifted(row_major(sums_of(grad_two, weight_two).astype(BF16)), "c", 1)
    mine = row_major((sums_of(grad_one, weight_one) + swap.astype(F32)).astype(BF16))
    own, left, right, far = (mine[src // 2 * k : src // 2 * (k + 1)] for k in range(nx))
    own = own.astype(F32)
    moved = [shifted(block, "x", by) for block, by in ((far, 2), (right, 1), (left, -1))]
    for block in moved:
        own = own + block.astype(F32)
    mine = own.astype(BF16)

    def by_core(mine, theirs):
        return jnp.where(core == 0, jnp.stack([mine, theirs]), jnp.stack([theirs, mine]))

    target_t, target_other, _ = lax.optimization_barrier((target_t, target_other, sent))
    target_both = by_core(target_t, target_other).astype(F32)
    w_both = by_core(w_mine, w_other).reshape(2 * cols, -1)
    squares = jnp.sum(target_both * target_both, axis=(0, 1))
    high = lax.reduce_precision(squares, 8, 7)
    extra = jnp.stack([high, squares - high]).astype(BF16)
    piece = jnp.concatenate([part_t, extra, jnp.zeros((6, nx * rows), BF16)], axis=0)
    every = told_all(piece, "y").reshape(HEADS // 2, part + 8, nx * rows)
    grad_t = every[:, :part].reshape(HEADS // 2 * part, nx * rows)
    squares_all = every[:, part : part + 2].astype(F32).sum(axis=(0, 1))
    inverse = lax.rsqrt(squares_all / WIDTH + EPS)
    normed_t = (target_both * inverse[None, None]).astype(BF16)
    weight_part = dot(normed_t.reshape(2 * cols, -1), grad_t, 1, 1).astype(BF16)

    weight_sent = weight_part.reshape(2, nz * nx, 8, -1).transpose(1, 0, 2, 3).reshape(nz * nx * 2, 8, -1)
    weight_got = exchanged(weight_sent, ("z", "x", "c"))
    weight_sum = weight_got.reshape(nz, nx * 2, 8, HEADS // 2 * part).astype(F32).sum(axis=0)
    gain_at = (lax.axis_index("z") * nx + x_at) * 8
    weight_sum = weight_sum * lax.dynamic_slice_in_dim(gain, gain_at, 8, 0)[None, :, None]
    weight_sum = lax.optimization_barrier(weight_sum).reshape(nx, 2, 8, HEADS // 2, part)
    grad_weight = weight_sum.transpose(2, 3, 1, 0, 4).reshape(8, WIDTH)

    grad_t, _ = lax.optimization_barrier((grad_t, weight_sent))
    rows_t = dot(w_both, grad_t, 1, 0)

    def rows_at(off):
        return lax.dynamic_slice_in_dim(rows_t, lax.rem(x_at + off, nx) * rows, rows, 1)

    rows_sum = rows_at(0)
    for off, by in ((1, 1), (3, -1), (2, 2)):
        rows_sum = rows_sum + shifted(rows_at(off).astype(BF16), "x", by).astype(F32)
    low, high = rows_sum[:cols], rows_sum[cols:]
    rows_in = shifted(jnp.where(core == 0, high, low).astype(BF16), "c", 1)
    grad_rows = (jnp.where(core == 0, low, high) + rows_in.astype(F32)).T.astype(BF16)

    mine, _ = lax.optimization_barrier((mine, weight_got))
    sums = exchanged(mine.reshape(ny, bit, 2 * HEAD_DIM), "y")
    sums = sums.reshape(KV_HEADS, 2, bit, 2, HEAD_DIM).astype(F32).sum(axis=1)
    sums = sums.transpose(2, 1, 0, 3).reshape(2, bit, KV_HEADS * HEAD_DIM)
    return (grad_rows, grad_weight, sums[0], sums[1])


def solution(mesh):
    finer = Mesh(mesh.devices.reshape(8, 4, 8, 2), ("z", "x", "y", "c"))
    sp, tp = ("z", "x"), ("y", "c")
    placed = (
        P(sp, tp),
        P(tp),
        P(tp, None),
        P(sp, tp),
        P(sp, None),
        P(sp, None),
        P(sp, tp),
        P(sp, tp),
    )

    return jax.shard_map(
        local,
        mesh=finer,
        in_specs=placed,
        out_specs=(P(sp, tp), P(tp + sp, None), P(sp + tp, None), P(sp + tp, None)),
        check_vma=False,
    )
```

```python
import jax
import jax.numpy as jnp
from jax import lax
from jax.experimental.layout import Layout, with_layout_constraint
from jax.sharding import Mesh
from jax.sharding import PartitionSpec as P

WIDTH = 4096
HEADS = 16
KV_HEADS = 4
HEAD_DIM = 256
EPS = 1e-06
SCALE = HEAD_DIM ** (-0.5)
F32 = jnp.float32
BF16 = jnp.bfloat16


def shifted(value, axis, by):
    n = lax.axis_size(axis)
    return lax.ppermute(value, axis, [(i, (i + by) % n) for i in range(n)])


def exchanged(value, axis):
    return lax.all_to_all(value, axis, split_axis=0, concat_axis=0, tiled=True)


def told_all(value, axis):
    n = lax.axis_size(axis)
    return exchanged(jnp.broadcast_to(value[None], (n, *value.shape)), axis)


def dot(a, b, ca, cb):
    return lax.dot_general(a, b, (((ca,), (cb,)), ((), ())), preferred_element_type=F32)


def row_major(value):
    return with_layout_constraint(value, Layout(major_to_minor=tuple(range(value.ndim))))


def terms(value):
    high = lax.reduce_precision(value, 8, 7)
    rest = value - high
    mid = lax.reduce_precision(rest, 8, 7)
    return [t.astype(BF16) for t in (high, mid, rest - mid)]


def local(target, gain, w_query, queries, keys, values, attn_out, grad_out):
    nz, nx, ny = lax.axis_size("z"), lax.axis_size("x"), lax.axis_size("y")
    rows, cols = queries.shape
    part = cols // nx
    src = keys.shape[0]
    bit = src // (2 * ny)
    core = lax.axis_index("c")
    x_at = lax.axis_index("x")
    kv = lax.axis_index("y") // 2
    n_rows = nz * rows

    delta_own = jnp.sum(attn_out.astype(F32) * grad_out.astype(F32), axis=1)
    line = jnp.concatenate(terms(delta_own) + [jnp.zeros((rows,), BF16)])[None]
    both = jnp.concatenate([queries, grad_out], axis=1)
    both = jnp.concatenate([both, line, jnp.zeros((7, 2 * cols), BF16)], axis=0)
    both = told_all(both, "z")

    def half_of(v):
        v = v.reshape(ny, 2, bit, v.shape[1])
        v = lax.dynamic_slice(v, (0, core, 0, kv * HEAD_DIM), (ny, 1, bit, HEAD_DIM))
        return v.reshape(src // 2, HEAD_DIM)

    pack = row_major(jnp.concatenate([half_of(keys), half_of(values), target], axis=0))
    blocks = [pack] + [shifted(pack, "x", by) for by in (1, -1, 2)]
    half = nx * src // 2
    target_all = jnp.zeros((nx * rows, cols), BF16)
    for block, off in zip(blocks, (0, 3, 1, 2)):
        target_all = lax.dynamic_update_slice(target_all, block[src:], (lax.rem(x_at + off, nx) * rows, 0))

    w_parts = lax.dynamic_slice(
        w_query.reshape(cols, HEADS // 2, 2, nx, part), (0, 0, 0, x_at, 0), (cols, HEADS // 2, 2, 1, part)
    )
    w_even = w_parts[:, :, 0].reshape(cols, -1)
    w_odd = w_parts[:, :, 1].reshape(cols, -1)
    w_mine = jnp.where(core == 0, w_even, w_odd)
    w_theirs = jnp.where(core == 0, w_odd, w_even)
    mine = [b[: src // 2] for b in blocks] + [b[src // 2 : src] for b in blocks]
    mine = row_major(jnp.concatenate(mine + [target_all, w_theirs[:, :cols], w_theirs[:, cols:]], axis=0))
    theirs = shifted(mine, "c", 1)
    key_one, value_one = mine[:half], mine[half : 2 * half]
    key_two, value_two = theirs[:half], theirs[half : 2 * half]

    both = both.reshape(nz, rows + 8, 2 * cols)
    query_all = both[:, :rows, :cols].reshape(n_rows, cols)
    grad_all = both[:, :rows, cols:].reshape(n_rows, cols)
    deltas = both[:, rows].astype(F32).reshape(nz, 4, rows).sum(axis=1).reshape(n_rows)
    score_one = dot(key_one, query_all, 1, 1) * SCALE
    score_two = dot(key_two, query_all, 1, 1) * SCALE
    peak = jnp.maximum(jnp.max(score_one, axis=0), jnp.max(score_two, axis=0))
    weight_one = jnp.exp(score_one - peak[None])
    weight_two = jnp.exp(score_two - peak[None])
    total = jnp.sum(weight_one, axis=0) + jnp.sum(weight_two, axis=0)
    weight_one, weight_two, total = lax.optimization_barrier(
        (weight_one.astype(BF16), weight_two.astype(BF16), total)
    )
    stats = told_all(jnp.concatenate([peak, total]).reshape(2 * nz, rows), "z").reshape(nz, 2, n_rows)

    def grads_of(weight, value):
        product = dot(value, grad_all, 1, 1)
        return (weight.astype(F32) * ((product - deltas[None]) * SCALE)).astype(BF16)

    grad_one = grads_of(weight_one, value_one)
    grad_two = grads_of(weight_two, value_two)
    query_t = dot(key_one, grad_one, 0, 0) + dot(key_two, grad_two, 0, 0)
    query_t, stats = lax.optimization_barrier((query_t, stats))
    top = jnp.max(stats[:, 0], axis=0)
    log_totals = top + jnp.log(jnp.sum(stats[:, 1] * jnp.exp(stats[:, 0] - top[None]), axis=0))
    share = jnp.exp(peak - log_totals)

    sent = (query_t * share[None]).astype(BF16).reshape(nx, part, nz, rows).transpose(2, 0, 1, 3)
    sent = sent.reshape(nz * nx, part, rows)
    got = exchanged(sent, ("z", "x")).reshape(nz, nx, part, rows)

    query_share, grad_share, _ = lax.optimization_barrier(
        ((query_all * share[:, None]).astype(BF16), (grad_all * share[:, None]).astype(BF16), sent)
    )

    def sums_of(grad, weight):
        return jnp.concatenate([dot(grad, query_share, 1, 0), dot(weight, grad_share, 1, 0)], axis=1)

    swap = shifted(row_major(sums_of(grad_two, weight_two).astype(BF16)), "c", 1)
    mine = row_major((sums_of(grad_one, weight_one) + swap.astype(F32)).astype(BF16))

    def by_core(mine, theirs):
        return jnp.where(core == 0, jnp.stack([mine, theirs]), jnp.stack([theirs, mine]))

    theirs, target_all, w_mine, _ = lax.optimization_barrier((theirs[2 * half :], target_all, w_mine, sent))
    target_other, w_other = theirs[: nx * rows], theirs[nx * rows :]
    w_other = jnp.concatenate([w_other[:cols], w_other[cols:]], axis=1)
    target_both = row_major(by_core(row_major(target_all.T), row_major(target_other.T)))
    w_both = by_core(w_mine, w_other).reshape(2 * cols, -1)
    squares = jnp.sum(jnp.square(target_both.astype(F32)), axis=(0, 1))

    got, mine, target_both = lax.optimization_barrier((got, mine, target_both))
    target_both = target_both.astype(F32)
    part_t = got.astype(F32).sum(axis=0)
    part_t = part_t.transpose(1, 0, 2).reshape(part, nx * rows).astype(BF16)
    own, left, right, far = (mine[src // 2 * k : src // 2 * (k + 1)] for k in range(nx))
    own = own.astype(F32)
    moved = [shifted(block, "x", by) for block, by in ((far, 2), (right, 1), (left, -1))]
    for block in moved:
        own = own + block.astype(F32)
    mine = own.astype(BF16)

    high = lax.reduce_precision(squares, 8, 7)
    extra = jnp.stack([high, squares - high]).astype(BF16)
    piece = jnp.concatenate([part_t, extra, jnp.zeros((6, nx * rows), BF16)], axis=0)
    every = told_all(piece, "y").reshape(HEADS // 2, part + 8, nx * rows)
    grad_t = every[:, :part].reshape(HEADS // 2 * part, nx * rows)
    squares_all = every[:, part : part + 2].astype(F32).sum(axis=(0, 1))
    inverse = lax.rsqrt(squares_all / WIDTH + EPS)
    normed_t = (target_both * inverse[None, None]).astype(BF16)
    weight_part = dot(normed_t.reshape(2 * cols, -1), grad_t, 1, 1).astype(BF16)

    weight_sent = weight_part.reshape(2, nz * nx, 8, -1).transpose(1, 0, 2, 3).reshape(nz * nx * 2, 8, -1)
    weight_got = exchanged(weight_sent, ("z", "x", "c"))
    weight_sum = weight_got.reshape(nz, nx * 2, 8, HEADS // 2 * part).astype(F32).sum(axis=0)
    gain_at = (lax.axis_index("z") * nx + x_at) * 8
    weight_sum = weight_sum * lax.dynamic_slice_in_dim(gain, gain_at, 8, 0)[None, :, None]
    weight_sum = lax.optimization_barrier(weight_sum).reshape(nx, 2, 8, HEADS // 2, part)
    grad_weight = weight_sum.transpose(2, 3, 1, 0, 4).reshape(8, WIDTH)

    grad_t, _ = lax.optimization_barrier((grad_t, weight_sent))
    rows_t = dot(w_both, grad_t, 1, 0)

    def rows_at(off):
        return lax.dynamic_slice_in_dim(rows_t, lax.rem(x_at + off, nx) * rows, rows, 1)

    rows_sum = rows_at(0)
    for off, by in ((1, 1), (3, -1), (2, 2)):
        rows_sum = rows_sum + shifted(rows_at(off).astype(BF16), "x", by).astype(F32)
    low, high = rows_sum[:cols], rows_sum[cols:]
    rows_in = shifted(jnp.where(core == 0, high, low).astype(BF16), "c", 1)
    grad_rows = (jnp.where(core == 0, low, high) + rows_in.astype(F32)).T.astype(BF16)

    mine, _ = lax.optimization_barrier((mine, weight_got))
    sums = exchanged(mine.reshape(ny, bit, 2 * HEAD_DIM), "y")
    sums = sums.reshape(KV_HEADS, 2, bit, 2, HEAD_DIM).astype(F32).sum(axis=1)
    sums = sums.transpose(2, 1, 0, 3).reshape(2, bit, KV_HEADS * HEAD_DIM)
    return (grad_rows, grad_weight, sums[0], sums[1])


def solution(mesh):
    finer = Mesh(mesh.devices.reshape(8, 4, 8, 2), ("z", "x", "y", "c"))
    sp, tp = ("z", "x"), ("y", "c")
    placed = (
        P(sp, tp),
        P(tp),
        P(tp, None),
        P(sp, tp),
        P(sp, None),
        P(sp, None),
        P(sp, tp),
        P(sp, tp),
    )

    return jax.shard_map(
        local,
        mesh=finer,
        in_specs=placed,
        out_specs=(P(sp, tp), P(tp + sp, None), P(sp + tp, None), P(sp + tp, None)),
        check_vma=False,
    )
```

```python
import jax
import jax.numpy as jnp
from jax import lax
from jax.experimental.layout import Layout, with_layout_constraint
from jax.sharding import Mesh
from jax.sharding import PartitionSpec as P

WIDTH = 4096
HEADS = 16
KV_HEADS = 4
HEAD_DIM = 256
EPS = 1e-06
SCALE = HEAD_DIM ** (-0.5)
F32 = jnp.float32
BF16 = jnp.bfloat16


def shifted(value, axis, by):
    n = lax.axis_size(axis)
    return lax.ppermute(value, axis, [(i, (i + by) % n) for i in range(n)])


def exchanged(value, axis):
    return lax.all_to_all(value, axis, split_axis=0, concat_axis=0, tiled=True)


def told_all(value, axis):
    n = lax.axis_size(axis)
    return exchanged(jnp.broadcast_to(value[None], (n, *value.shape)), axis)


def dot(a, b, ca, cb):
    return lax.dot_general(a, b, (((ca,), (cb,)), ((), ())), preferred_element_type=F32)


def row_major(value):
    return with_layout_constraint(value, Layout(major_to_minor=tuple(range(value.ndim))))


def terms(value):
    high = lax.reduce_precision(value, 8, 7)
    rest = value - high
    mid = lax.reduce_precision(rest, 8, 7)
    return [t.astype(BF16) for t in (high, mid, rest - mid)]


def local(target, gain, w_query, queries, keys, values, attn_out, grad_out):
    nz, nx, ny = lax.axis_size("z"), lax.axis_size("x"), lax.axis_size("y")
    rows, cols = queries.shape
    part = cols // nx
    src = keys.shape[0]
    bit = src // (2 * ny)
    core = lax.axis_index("c")
    x_at = lax.axis_index("x")
    kv = lax.axis_index("y") // 2
    n_rows = nz * rows

    delta_own = jnp.sum(attn_out.astype(F32) * grad_out.astype(F32), axis=1)
    line = jnp.concatenate(terms(delta_own) + [jnp.zeros((rows,), BF16)])[None]
    both = jnp.concatenate([queries, grad_out], axis=1)
    both = jnp.concatenate([both, line, jnp.zeros((7, 2 * cols), BF16)], axis=0)
    both = told_all(both, "z")

    def half_of(v):
        v = v.reshape(ny, 2, bit, v.shape[1])
        v = lax.dynamic_slice(v, (0, core, 0, kv * HEAD_DIM), (ny, 1, bit, HEAD_DIM))
        return v.reshape(src // 2, HEAD_DIM)

    pack = row_major(jnp.concatenate([half_of(keys), half_of(values), target], axis=0))
    blocks = [pack] + [shifted(pack, "x", by) for by in (1, -1, 2)]
    target_all = jnp.zeros((nx * rows, cols), BF16)
    for block, off in zip(blocks, (0, 3, 1, 2)):
        target_all = lax.dynamic_update_slice(target_all, block[src:], (lax.rem(x_at + off, nx) * rows, 0))

    w_parts = lax.dynamic_slice(
        w_query.reshape(cols, HEADS // 2, 2, nx, part), (0, 0, 0, x_at, 0), (cols, HEADS // 2, 2, 1, part)
    )
    w_even = w_parts[:, :, 0].reshape(cols, -1)
    w_odd = w_parts[:, :, 1].reshape(cols, -1)
    w_mine = jnp.where(core == 0, w_even, w_odd)
    w_theirs = jnp.where(core == 0, w_odd, w_even)
    swap = [b[:src] for b in blocks] + [target_all, w_theirs[:, :cols], w_theirs[:, cols:]]
    swap = shifted(row_major(jnp.concatenate(swap, axis=0)), "c", 1)
    blocks = [b[:src] for b in blocks] + [swap[src * k : src * (k + 1)] for k in range(nx)]
    key_all = row_major(jnp.concatenate([b[: src // 2] for b in blocks], axis=0))
    value_all = row_major(jnp.concatenate([b[src // 2 :] for b in blocks], axis=0))
    target_other = swap[nx * src : nx * src + nx * rows]
    w_other = swap[nx * src + nx * rows :]
    w_other = jnp.concatenate([w_other[:cols], w_other[cols:]], axis=1)

    both = both.reshape(nz, rows + 8, 2 * cols)
    query_all = both[:, :rows, :cols].reshape(n_rows, cols)
    grad_all = both[:, :rows, cols:].reshape(n_rows, cols)
    deltas = both[:, rows].astype(F32).reshape(nz, 4, rows).sum(axis=1).reshape(n_rows)
    scores = dot(key_all, query_all, 1, 1) * SCALE
    peak = jnp.max(scores, axis=0)
    weights = jnp.exp(scores - peak[None])
    total = jnp.sum(weights, axis=0)
    stats = told_all(jnp.concatenate([peak, total]).reshape(2 * nz, rows), "z").reshape(nz, 2, n_rows)
    grad_weights = dot(value_all, grad_all, 1, 1)
    grad_scores = (weights * ((grad_weights - deltas[None]) * SCALE)).astype(BF16)
    query_t = dot(key_all, grad_scores, 0, 0)
    query_t, stats = lax.optimization_barrier((query_t, stats))
    top = jnp.max(stats[:, 0], axis=0)
    log_totals = top + jnp.log(jnp.sum(stats[:, 1] * jnp.exp(stats[:, 0] - top[None]), axis=0))
    share = jnp.exp(peak - log_totals)

    sent = (query_t * share[None]).astype(BF16).reshape(nx, part, nz, rows).transpose(2, 0, 1, 3)
    sent = sent.reshape(nz * nx, part, rows)
    got = exchanged(sent, ("z", "x")).reshape(nz, nx, part, rows)
    part_t = got.astype(F32).sum(axis=0)
    part_t = part_t.transpose(1, 0, 2).reshape(part, nx * rows).astype(BF16)

    query_share, grad_share, _ = lax.optimization_barrier(
        ((query_all * share[:, None]).astype(BF16), (grad_all * share[:, None]).astype(BF16), sent)
    )
    key_sum = dot(grad_scores, query_share, 1, 0)
    value_sum = dot(weights.astype(BF16), grad_share, 1, 0)
    half = nx * src // 2
    theirs = jnp.concatenate([key_sum[half:], value_sum[half:]], axis=1).astype(BF16)
    mine = jnp.concatenate([key_sum[:half], value_sum[:half]], axis=1)
    mine = row_major((mine + shifted(row_major(theirs), "c", 1).astype(F32)).astype(BF16))
    own, left, right, far = (mine[src // 2 * k : src // 2 * (k + 1)] for k in range(nx))
    own = own.astype(F32)
    moved = [shifted(block, "x", by) for block, by in ((far, 2), (right, 1), (left, -1))]
    for block in moved:
        own = own + block.astype(F32)
    mine = own.astype(BF16)

    def by_core(mine, theirs):
        return jnp.where(core == 0, jnp.stack([mine, theirs]), jnp.stack([theirs, mine]))

    target_both = by_core(target_all.T, target_other.T).astype(F32)
    w_both = by_core(w_mine, w_other).reshape(2 * cols, -1)
    squares = jnp.sum(target_both * target_both, axis=(0, 1))
    high = lax.reduce_precision(squares, 8, 7)
    extra = jnp.stack([high, squares - high]).astype(BF16)
    piece = jnp.concatenate([part_t, extra, jnp.zeros((6, nx * rows), BF16)], axis=0)
    every = told_all(piece, "y").reshape(HEADS // 2, part + 8, nx * rows)
    grad_t = every[:, :part].reshape(HEADS // 2 * part, nx * rows)
    squares_all = every[:, part : part + 2].astype(F32).sum(axis=(0, 1))
    inverse = lax.rsqrt(squares_all / WIDTH + EPS)
    normed_t = (target_both * inverse[None, None]).astype(BF16)
    weight_part = dot(normed_t.reshape(2 * cols, -1), grad_t, 1, 1).astype(BF16)

    weight_sent = weight_part.reshape(2, nz * nx, 8, -1).transpose(1, 0, 2, 3).reshape(nz * nx * 2, 8, -1)
    weight_got = exchanged(weight_sent, ("z", "x", "c"))
    weight_sum = weight_got.reshape(nz, nx * 2, 8, HEADS // 2 * part).astype(F32).sum(axis=0)
    gain_at = (lax.axis_index("z") * nx + x_at) * 8
    weight_sum = weight_sum * lax.dynamic_slice_in_dim(gain, gain_at, 8, 0)[None, :, None]
    weight_sum = lax.optimization_barrier(weight_sum).reshape(nx, 2, 8, HEADS // 2, part)
    grad_weight = weight_sum.transpose(2, 3, 1, 0, 4).reshape(8, WIDTH)

    grad_t, _ = lax.optimization_barrier((grad_t, weight_sent))
    rows_t = dot(w_both, grad_t, 1, 0)

    def rows_at(off):
        return lax.dynamic_slice_in_dim(rows_t, lax.rem(x_at + off, nx) * rows, rows, 1)

    rows_sum = rows_at(0)
    for off, by in ((1, 1), (3, -1), (2, 2)):
        rows_sum = rows_sum + shifted(rows_at(off).astype(BF16), "x", by).astype(F32)
    low, high = rows_sum[:cols], rows_sum[cols:]
    rows_in = shifted(jnp.where(core == 0, high, low).astype(BF16), "c", 1)
    grad_rows = (jnp.where(core == 0, low, high) + rows_in.astype(F32)).T.astype(BF16)

    mine, _ = lax.optimization_barrier((mine, weight_got))
    sums = exchanged(mine.reshape(ny, bit, 2 * HEAD_DIM), "y")
    sums = sums.reshape(KV_HEADS, 2, bit, 2, HEAD_DIM).astype(F32).sum(axis=1)
    sums = sums.transpose(2, 1, 0, 3).reshape(2, bit, KV_HEADS * HEAD_DIM)
    return (grad_rows, grad_weight, sums[0], sums[1])


def solution(mesh):
    finer = Mesh(mesh.devices.reshape(8, 4, 8, 2), ("z", "x", "y", "c"))
    sp, tp = ("z", "x"), ("y", "c")
    placed = (
        P(sp, tp),
        P(tp),
        P(tp, None),
        P(sp, tp),
        P(sp, None),
        P(sp, None),
        P(sp, tp),
        P(sp, tp),
    )

    return jax.shard_map(
        local,
        mesh=finer,
        in_specs=placed,
        out_specs=(P(sp, tp), P(tp + sp, None), P(sp + tp, None), P(sp + tp, None)),
        check_vma=False,
    )
```

```python
import jax
import jax.numpy as jnp
from jax import lax
from jax.experimental.layout import Layout, with_layout_constraint
from jax.sharding import Mesh
from jax.sharding import PartitionSpec as P

WIDTH = 4096
HEADS = 16
KV_HEADS = 4
HEAD_DIM = 256
EPS = 1e-06
SCALE = HEAD_DIM ** (-0.5)
F32 = jnp.float32
BF16 = jnp.bfloat16


def shifted(value, axis, by):
    n = lax.axis_size(axis)
    return lax.ppermute(value, axis, [(i, (i + by) % n) for i in range(n)])


def exchanged(value, axis):
    return lax.all_to_all(value, axis, split_axis=0, concat_axis=0, tiled=True)


def told_all(value, axis):
    n = lax.axis_size(axis)
    return exchanged(jnp.broadcast_to(value[None], (n, *value.shape)), axis)


def dot(a, b, ca, cb):
    return lax.dot_general(a, b, (((ca,), (cb,)), ((), ())), preferred_element_type=F32)


def row_major(value):
    return with_layout_constraint(value, Layout(major_to_minor=tuple(range(value.ndim))))


def terms(value):
    high = lax.reduce_precision(value, 8, 7)
    rest = value - high
    mid = lax.reduce_precision(rest, 8, 7)
    return [t.astype(BF16) for t in (high, mid, rest - mid)]


def local(target, gain, w_query, queries, keys, values, attn_out, grad_out):
    nz, nx, ny = lax.axis_size("z"), lax.axis_size("x"), lax.axis_size("y")
    rows, cols = queries.shape
    part = cols // nx
    src = keys.shape[0]
    bit = src // (2 * ny)
    core = lax.axis_index("c")
    x_at = lax.axis_index("x")
    kv = lax.axis_index("y") // 2
    n_rows = nz * rows

    delta_own = jnp.sum(attn_out.astype(F32) * grad_out.astype(F32), axis=1)
    line = jnp.concatenate(terms(delta_own) + [jnp.zeros((rows,), BF16)])[None]
    both = jnp.concatenate([queries, grad_out], axis=1)
    both = jnp.concatenate([both, line, jnp.zeros((7, 2 * cols), BF16)], axis=0)
    both = told_all(both, "z")

    def half_of(v):
        v = v.reshape(ny, 2, bit, v.shape[1])
        v = lax.dynamic_slice(v, (0, core, 0, kv * HEAD_DIM), (ny, 1, bit, HEAD_DIM))
        return v.reshape(src // 2, HEAD_DIM)

    pack = row_major(jnp.concatenate([half_of(keys), half_of(values), target], axis=0))
    blocks = [pack] + [shifted(pack, "x", by) for by in (1, -1, 2)]
    target_all = jnp.zeros((nx * rows, cols), BF16)
    for block, off in zip(blocks, (0, 3, 1, 2)):
        target_all = lax.dynamic_update_slice(target_all, block[src:], (lax.rem(x_at + off, nx) * rows, 0))

    swap = [b[:src] for b in blocks] + [target_all]
    swap = shifted(row_major(jnp.concatenate(swap, axis=0)), "c", 1)
    blocks = [b[:src] for b in blocks] + [swap[src * k : src * (k + 1)] for k in range(nx)]
    key_all = row_major(jnp.concatenate([b[: src // 2] for b in blocks], axis=0))
    value_all = row_major(jnp.concatenate([b[src // 2 :] for b in blocks], axis=0))
    target_other = swap[nx * src :]

    both = both.reshape(nz, rows + 8, 2 * cols)
    query_all = both[:, :rows, :cols].reshape(n_rows, cols)
    grad_all = both[:, :rows, cols:].reshape(n_rows, cols)
    deltas = both[:, rows].astype(F32).reshape(nz, 4, rows).sum(axis=1).reshape(n_rows)
    scores = dot(key_all, query_all, 1, 1) * SCALE
    peak = jnp.max(scores, axis=0)
    weights = jnp.exp(scores - peak[None])
    total = jnp.sum(weights, axis=0)
    stats = told_all(jnp.concatenate([peak, total]).reshape(2 * nz, rows), "z").reshape(nz, 2, n_rows)
    grad_weights = dot(value_all, grad_all, 1, 1)
    grad_scores = (weights * ((grad_weights - deltas[None]) * SCALE)).astype(BF16)
    query_t = dot(key_all, grad_scores, 0, 0)
    query_t, stats = lax.optimization_barrier((query_t, stats))
    top = jnp.max(stats[:, 0], axis=0)
    log_totals = top + jnp.log(jnp.sum(stats[:, 1] * jnp.exp(stats[:, 0] - top[None]), axis=0))
    share = jnp.exp(peak - log_totals)

    sent = (query_t * share[None]).astype(BF16).reshape(nx, part, nz, rows).transpose(2, 0, 1, 3)
    sent = sent.reshape(nz * nx, part, rows)
    got = exchanged(sent, ("z", "x")).reshape(nz, nx, part, rows)
    part_t = got.astype(F32).sum(axis=0)
    part_t = part_t.transpose(1, 0, 2).reshape(part, nx * rows).astype(BF16)

    query_share, grad_share, _ = lax.optimization_barrier(
        ((query_all * share[:, None]).astype(BF16), (grad_all * share[:, None]).astype(BF16), sent)
    )
    key_sum = dot(grad_scores, query_share, 1, 0)
    value_sum = dot(weights.astype(BF16), grad_share, 1, 0)
    half = nx * src // 2
    theirs = jnp.concatenate([key_sum[half:], value_sum[half:]], axis=1).astype(BF16)
    mine = jnp.concatenate([key_sum[:half], value_sum[:half]], axis=1)
    mine = row_major((mine + shifted(row_major(theirs), "c", 1).astype(F32)).astype(BF16))
    own, left, right, far = (mine[src // 2 * k : src // 2 * (k + 1)] for k in range(nx))
    own = own.astype(F32)
    moved = [shifted(block, "x", by) for block, by in ((far, 2), (right, 1), (left, -1))]
    for block in moved:
        own = own + block.astype(F32)
    mine = own.astype(BF16)

    def by_core(mine, theirs):
        return jnp.where(core == 0, jnp.stack([mine, theirs]), jnp.stack([theirs, mine]))

    target_both = by_core(target_all.T, target_other.T).astype(F32)
    squares = jnp.sum(target_both * target_both, axis=(0, 1))
    high = lax.reduce_precision(squares, 8, 7)
    extra = jnp.stack([high, squares - high]).astype(BF16)
    piece = jnp.concatenate([part_t, extra, jnp.zeros((6, nx * rows), BF16)], axis=0)
    every = told_all(piece, "y").reshape(HEADS // 2, part + 8, nx * rows)
    grad_t = every[:, :part].reshape(HEADS // 2 * part, nx * rows)
    squares_all = every[:, part : part + 2].astype(F32).sum(axis=(0, 1))
    inverse = lax.rsqrt(squares_all / WIDTH + EPS)
    normed_t = (target_both * inverse[None, None]).astype(BF16)
    weight_part = dot(normed_t.reshape(2 * cols, -1), grad_t, 1, 1).astype(BF16)

    weight_sent = weight_part.reshape(2, nz * nx, 8, -1).transpose(1, 0, 2, 3).reshape(nz * nx * 2, 8, -1)
    weight_got = exchanged(weight_sent, ("z", "x", "c"))
    weight_sum = weight_got.reshape(nz, nx * 2, 8, HEADS // 2 * part).astype(F32).sum(axis=0)
    gain_at = (lax.axis_index("z") * nx + x_at) * 8
    weight_sum = weight_sum * lax.dynamic_slice_in_dim(gain, gain_at, 8, 0)[None, :, None]
    weight_sum = lax.optimization_barrier(weight_sum).reshape(nx, 2, 8, HEADS // 2, part)
    grad_weight = weight_sum.transpose(2, 3, 1, 0, 4).reshape(8, WIDTH)

    w_late, _ = lax.optimization_barrier((w_query, sent))
    w_parts = lax.dynamic_slice(
        w_late.reshape(cols, HEADS // 2, 2, nx, part), (0, 0, 0, x_at, 0), (cols, HEADS // 2, 2, 1, part)
    )
    w_even = w_parts[:, :, 0].reshape(cols, -1)
    w_odd = w_parts[:, :, 1].reshape(cols, -1)
    w_mine = jnp.where(core == 0, w_even, w_odd)
    w_theirs = jnp.where(core == 0, w_odd, w_even)
    grad_t, _ = lax.optimization_barrier((grad_t, weight_sent))
    grad_other = shifted(grad_t, "c", 1)
    rows_t = dot(w_mine, grad_t, 1, 0) + dot(w_theirs, grad_other, 1, 0)

    def rows_at(off):
        return lax.dynamic_slice_in_dim(rows_t, lax.rem(x_at + off, nx) * rows, rows, 1)

    rows_sum = rows_at(0)
    for off, by in ((1, 1), (3, -1), (2, 2)):
        rows_sum = rows_sum + shifted(rows_at(off).astype(BF16), "x", by).astype(F32)
    grad_rows = rows_sum.T.astype(BF16)

    mine, _ = lax.optimization_barrier((mine, weight_got))
    sums = exchanged(mine.reshape(ny, bit, 2 * HEAD_DIM), "y")
    sums = sums.reshape(KV_HEADS, 2, bit, 2, HEAD_DIM).astype(F32).sum(axis=1)
    sums = sums.transpose(2, 1, 0, 3).reshape(2, bit, KV_HEADS * HEAD_DIM)
    return (grad_rows, grad_weight, sums[0], sums[1])


def solution(mesh):
    finer = Mesh(mesh.devices.reshape(8, 4, 8, 2), ("z", "x", "y", "c"))
    sp, tp = ("z", "x"), ("y", "c")
    placed = (
        P(sp, tp),
        P(tp),
        P(tp, None),
        P(sp, tp),
        P(sp, None),
        P(sp, None),
        P(sp, tp),
        P(sp, tp),
    )

    return jax.shard_map(
        local,
        mesh=finer,
        in_specs=placed,
        out_specs=(P(sp, tp), P(tp + sp, None), P(sp + tp, None), P(sp + tp, None)),
        check_vma=False,
    )
```

```python
import jax
import jax.numpy as jnp
from jax import lax
from jax.experimental.layout import Layout, with_layout_constraint
from jax.sharding import Mesh
from jax.sharding import PartitionSpec as P

WIDTH = 4096
HEADS = 16
KV_HEADS = 4
HEAD_DIM = 256
EPS = 1e-06
SCALE = HEAD_DIM ** (-0.5)
F32 = jnp.float32
BF16 = jnp.bfloat16


def shifted(value, axis, by):
    n = lax.axis_size(axis)
    return lax.ppermute(value, axis, [(i, (i + by) % n) for i in range(n)])


def exchanged(value, axis):
    return lax.all_to_all(value, axis, split_axis=0, concat_axis=0, tiled=True)


def told_all(value, axis):
    n = lax.axis_size(axis)
    return exchanged(jnp.broadcast_to(value[None], (n, *value.shape)), axis)


def dot(a, b, ca, cb):
    return lax.dot_general(a, b, (((ca,), (cb,)), ((), ())), preferred_element_type=F32)


def row_major(value):
    return with_layout_constraint(value, Layout(major_to_minor=tuple(range(value.ndim))))


def terms(value):
    high = lax.reduce_precision(value, 8, 7)
    rest = value - high
    mid = lax.reduce_precision(rest, 8, 7)
    return [t.astype(BF16) for t in (high, mid, rest - mid)]


def local(target, gain, w_query, queries, keys, values, attn_out, grad_out):
    nz, nx, ny = lax.axis_size("z"), lax.axis_size("x"), lax.axis_size("y")
    rows, cols = queries.shape
    part = cols // nx
    src = keys.shape[0]
    bit = src // (2 * ny)
    core = lax.axis_index("c")
    x_at = lax.axis_index("x")
    kv = lax.axis_index("y") // 2
    n_rows = nz * rows

    delta_own = jnp.sum(attn_out.astype(F32) * grad_out.astype(F32), axis=1)
    line = jnp.concatenate(terms(delta_own) + [jnp.zeros((rows,), BF16)])[None]
    both = jnp.concatenate([queries, grad_out], axis=1)
    both = jnp.concatenate([both, line, jnp.zeros((7, 2 * cols), BF16)], axis=0)
    both = told_all(both, "z")

    def half_of(v):
        v = v.reshape(ny, 2, bit, v.shape[1])
        v = lax.dynamic_slice(v, (0, core, 0, kv * HEAD_DIM), (ny, 1, bit, HEAD_DIM))
        return v.reshape(src // 2, HEAD_DIM)

    pack = row_major(jnp.concatenate([half_of(keys), half_of(values), target], axis=0))
    blocks = [pack] + [shifted(pack, "x", by) for by in (1, -1, 2)]
    target_all = jnp.zeros((nx * rows, cols), BF16)
    for block, off in zip(blocks, (0, 3, 1, 2)):
        target_all = lax.dynamic_update_slice(target_all, block[src:], (lax.rem(x_at + off, nx) * rows, 0))

    w_parts = lax.dynamic_slice(
        w_query.reshape(cols, HEADS // 2, 2, nx, part), (0, 0, 0, x_at, 0), (cols, HEADS // 2, 2, 1, part)
    )
    w_even = w_parts[:, :, 0].reshape(cols, -1)
    w_odd = w_parts[:, :, 1].reshape(cols, -1)
    w_mine = jnp.where(core == 0, w_even, w_odd)
    w_theirs = jnp.where(core == 0, w_odd, w_even)

    half = nx * src // 2
    mine = [b[: src // 2] for b in blocks] + [b[src // 2 : src] for b in blocks] + [target_all]
    mine = row_major(jnp.concatenate(mine, axis=0))
    mine, w_mine, w_theirs = lax.optimization_barrier((mine, w_mine, w_theirs))
    theirs = shifted(mine, "c", 1)
    target_other = theirs[2 * half :]
    key_one, value_one = mine[:half], mine[half : 2 * half]
    key_two, value_two = theirs[:half], theirs[half : 2 * half]

    both = both.reshape(nz, rows + 8, 2 * cols)
    query_all = both[:, :rows, :cols].reshape(n_rows, cols)
    grad_all = both[:, :rows, cols:].reshape(n_rows, cols)
    deltas = both[:, rows].astype(F32).reshape(nz, 4, rows).sum(axis=1).reshape(n_rows)
    score_one = dot(key_one, query_all, 1, 1) * SCALE
    score_two = dot(key_two, query_all, 1, 1) * SCALE
    peak = jnp.maximum(jnp.max(score_one, axis=0), jnp.max(score_two, axis=0))
    weight_one = jnp.exp(score_one - peak[None])
    weight_two = jnp.exp(score_two - peak[None])
    total = jnp.sum(weight_one, axis=0) + jnp.sum(weight_two, axis=0)
    weight_one, weight_two, total = lax.optimization_barrier(
        (weight_one.astype(BF16), weight_two.astype(BF16), total)
    )
    stats = told_all(jnp.concatenate([peak, total]).reshape(2 * nz, rows), "z").reshape(nz, 2, n_rows)

    def grads_of(weight, value):
        product = dot(value, grad_all, 1, 1)
        return (weight.astype(F32) * ((product - deltas[None]) * SCALE)).astype(BF16)

    grad_one = grads_of(weight_one, value_one)
    grad_two = grads_of(weight_two, value_two)
    query_t = dot(key_one, grad_one, 0, 0) + dot(key_two, grad_two, 0, 0)
    query_t, stats = lax.optimization_barrier((query_t, stats))
    top = jnp.max(stats[:, 0], axis=0)
    log_totals = top + jnp.log(jnp.sum(stats[:, 1] * jnp.exp(stats[:, 0] - top[None]), axis=0))
    share = jnp.exp(peak - log_totals)

    sent = (query_t * share[None]).astype(BF16).reshape(nx, part, nz, rows).transpose(2, 0, 1, 3)
    sent = sent.reshape(nz * nx, part, rows)
    got = exchanged(sent, ("z", "x")).reshape(nz, nx, part, rows)
    part_t = got.astype(F32).sum(axis=0)
    part_t = part_t.transpose(1, 0, 2).reshape(part, nx * rows).astype(BF16)

    query_share, grad_share, _ = lax.optimization_barrier(
        ((query_all * share[:, None]).astype(BF16), (grad_all * share[:, None]).astype(BF16), sent)
    )

    def sums_of(grad, weight):
        return jnp.concatenate([dot(grad, query_share, 1, 0), dot(weight, grad_share, 1, 0)], axis=1)

    swap = shifted(row_major(sums_of(grad_two, weight_two).astype(BF16)), "c", 1)
    mine = row_major((sums_of(grad_one, weight_one) + swap.astype(F32)).astype(BF16))
    own, left, right, far = (mine[src // 2 * k : src // 2 * (k + 1)] for k in range(nx))
    own = own.astype(F32)
    moved = [shifted(block, "x", by) for block, by in ((far, 2), (right, 1), (left, -1))]
    for block in moved:
        own = own + block.astype(F32)
    mine = own.astype(BF16)

    def by_core(mine, theirs):
        return jnp.where(core == 0, jnp.stack([mine, theirs]), jnp.stack([theirs, mine]))

    target_both = by_core(target_all.T, target_other.T).astype(F32)
    squares = jnp.sum(target_both * target_both, axis=(0, 1))
    high = lax.reduce_precision(squares, 8, 7)
    extra = jnp.stack([high, squares - high]).astype(BF16)
    piece = jnp.concatenate([part_t, extra, jnp.zeros((6, nx * rows), BF16)], axis=0)
    every = told_all(piece, "y").reshape(HEADS // 2, part + 8, nx * rows)
    grad_t = every[:, :part].reshape(HEADS // 2 * part, nx * rows)
    squares_all = every[:, part : part + 2].astype(F32).sum(axis=(0, 1))
    inverse = lax.rsqrt(squares_all / WIDTH + EPS)
    normed_t = (target_both * inverse[None, None]).astype(BF16)
    weight_part = dot(normed_t.reshape(2 * cols, -1), grad_t, 1, 1).astype(BF16)

    weight_sent = weight_part.reshape(2, nz * nx, 8, -1).transpose(1, 0, 2, 3).reshape(nz * nx * 2, 8, -1)
    weight_got = exchanged(weight_sent, ("z", "x", "c"))
    weight_sum = weight_got.reshape(nz, nx * 2, 8, HEADS // 2 * part).astype(F32).sum(axis=0)
    gain_at = (lax.axis_index("z") * nx + x_at) * 8
    weight_sum = weight_sum * lax.dynamic_slice_in_dim(gain, gain_at, 8, 0)[None, :, None]
    weight_sum = lax.optimization_barrier(weight_sum).reshape(nx, 2, 8, HEADS // 2, part)
    grad_weight = weight_sum.transpose(2, 3, 1, 0, 4).reshape(8, WIDTH)

    grad_t, _ = lax.optimization_barrier((grad_t, weight_sent))
    grad_other = shifted(grad_t, "c", 1)
    rows_t = dot(w_mine, grad_t, 1, 0) + dot(w_theirs, grad_other, 1, 0)

    def rows_at(off):
        return lax.dynamic_slice_in_dim(rows_t, lax.rem(x_at + off, nx) * rows, rows, 1)

    rows_sum = rows_at(0)
    for off, by in ((1, 1), (3, -1), (2, 2)):
        rows_sum = rows_sum + shifted(rows_at(off).astype(BF16), "x", by).astype(F32)
    grad_rows = rows_sum.T.astype(BF16)

    mine, _ = lax.optimization_barrier((mine, weight_got))
    sums = exchanged(mine.reshape(ny, bit, 2 * HEAD_DIM), "y")
    sums = sums.reshape(KV_HEADS, 2, bit, 2, HEAD_DIM).astype(F32).sum(axis=1)
    sums = sums.transpose(2, 1, 0, 3).reshape(2, bit, KV_HEADS * HEAD_DIM)
    return (grad_rows, grad_weight, sums[0], sums[1])


def solution(mesh):
    finer = Mesh(mesh.devices.reshape(8, 4, 8, 2), ("z", "x", "y", "c"))
    sp, tp = ("z", "x"), ("y", "c")
    placed = (
        P(sp, tp),
        P(tp),
        P(tp, None),
        P(sp, tp),
        P(sp, None),
        P(sp, None),
        P(sp, tp),
        P(sp, tp),
    )

    return jax.shard_map(
        local,
        mesh=finer,
        in_specs=placed,
        out_specs=(P(sp, tp), P(tp + sp, None), P(sp + tp, None), P(sp + tp, None)),
        check_vma=False,
    )
```

```python
import jax
import jax.numpy as jnp
from jax import lax
from jax.experimental.layout import Layout, with_layout_constraint
from jax.sharding import Mesh
from jax.sharding import PartitionSpec as P

WIDTH = 4096
HEADS = 16
KV_HEADS = 4
HEAD_DIM = 256
EPS = 1e-06
SCALE = HEAD_DIM ** (-0.5)
F32 = jnp.float32
BF16 = jnp.bfloat16


def shifted(value, axis, by):
    n = lax.axis_size(axis)
    return lax.ppermute(value, axis, [(i, (i + by) % n) for i in range(n)])


def exchanged(value, axis):
    return lax.all_to_all(value, axis, split_axis=0, concat_axis=0, tiled=True)


def told_all(value, axis):
    n = lax.axis_size(axis)
    return exchanged(jnp.broadcast_to(value[None], (n, *value.shape)), axis)


def dot(a, b, ca, cb):
    return lax.dot_general(a, b, (((ca,), (cb,)), ((), ())), preferred_element_type=F32)


def row_major(value):
    return with_layout_constraint(value, Layout(major_to_minor=tuple(range(value.ndim))))


def terms(value):
    high = lax.reduce_precision(value, 8, 7)
    rest = value - high
    mid = lax.reduce_precision(rest, 8, 7)
    return [t.astype(BF16) for t in (high, mid, rest - mid)]


def local(target, gain, w_query, queries, keys, values, attn_out, grad_out):
    nz, nx, ny = lax.axis_size("z"), lax.axis_size("x"), lax.axis_size("y")
    rows, cols = queries.shape
    part = cols // nx
    src = keys.shape[0]
    bit = src // (2 * ny)
    core = lax.axis_index("c")
    x_at = lax.axis_index("x")
    kv = lax.axis_index("y") // 2
    n_rows = nz * rows

    delta_own = jnp.sum(attn_out.astype(F32) * grad_out.astype(F32), axis=1)
    line = jnp.concatenate(terms(delta_own) + [jnp.zeros((rows,), BF16)])[None]
    both = jnp.concatenate([queries, grad_out], axis=1)
    both = jnp.concatenate([both, line, jnp.zeros((7, 2 * cols), BF16)], axis=0)
    both = told_all(both, "z")

    def half_of(v):
        v = v.reshape(ny, 2, bit, v.shape[1])
        v = lax.dynamic_slice(v, (0, core, 0, kv * HEAD_DIM), (ny, 1, bit, HEAD_DIM))
        return v.reshape(src // 2, HEAD_DIM)

    pack = row_major(jnp.concatenate([half_of(keys), half_of(values), target], axis=0))
    blocks = [pack] + [shifted(pack, "x", by) for by in (1, -1, 2)]
    target_all = jnp.zeros((nx * rows, cols), BF16)
    for block, off in zip(blocks, (0, 3, 1, 2)):
        target_all = lax.dynamic_update_slice(target_all, block[src:], (lax.rem(x_at + off, nx) * rows, 0))

    w_parts = lax.dynamic_slice(
        w_query.reshape(cols, HEADS // 2, 2, nx, part), (0, 0, 0, x_at, 0), (cols, HEADS // 2, 2, 1, part)
    )
    w_even = w_parts[:, :, 0].reshape(cols, -1)
    w_odd = w_parts[:, :, 1].reshape(cols, -1)
    w_mine = jnp.where(core == 0, w_even, w_odd)
    w_theirs = jnp.where(core == 0, w_odd, w_even)

    half = nx * src // 2
    mine = [b[: src // 2] for b in blocks] + [b[src // 2 : src] for b in blocks]
    mine = row_major(jnp.concatenate(mine, axis=0))
    mine, w_mine, w_theirs = lax.optimization_barrier((mine, w_mine, w_theirs))
    theirs = shifted(mine, "c", 1)
    key_one, value_one = mine[:half], mine[half : 2 * half]
    key_two, value_two = theirs[:half], theirs[half : 2 * half]

    both = both.reshape(nz, rows + 8, 2 * cols)
    query_all = both[:, :rows, :cols].reshape(n_rows, cols)
    grad_all = both[:, :rows, cols:].reshape(n_rows, cols)
    deltas = both[:, rows].astype(F32).reshape(nz, 4, rows).sum(axis=1).reshape(n_rows)
    score_one = dot(key_one, query_all, 1, 1) * SCALE
    score_two = dot(key_two, query_all, 1, 1) * SCALE
    peak = jnp.maximum(jnp.max(score_one, axis=0), jnp.max(score_two, axis=0))
    weight_one = jnp.exp(score_one - peak[None])
    weight_two = jnp.exp(score_two - peak[None])
    total = jnp.sum(weight_one, axis=0) + jnp.sum(weight_two, axis=0)
    weight_one, weight_two, total = lax.optimization_barrier(
        (weight_one.astype(BF16), weight_two.astype(BF16), total)
    )
    stats = told_all(jnp.concatenate([peak, total]).reshape(2 * nz, rows), "z").reshape(nz, 2, n_rows)

    def grads_of(weight, value):
        product = dot(value, grad_all, 1, 1)
        return (weight.astype(F32) * ((product - deltas[None]) * SCALE)).astype(BF16)

    grad_one = grads_of(weight_one, value_one)
    grad_two = grads_of(weight_two, value_two)
    query_t = dot(key_one, grad_one, 0, 0) + dot(key_two, grad_two, 0, 0)
    query_t, stats = lax.optimization_barrier((query_t, stats))
    top = jnp.max(stats[:, 0], axis=0)
    log_totals = top + jnp.log(jnp.sum(stats[:, 1] * jnp.exp(stats[:, 0] - top[None]), axis=0))
    share = jnp.exp(peak - log_totals)

    sent = (query_t * share[None]).astype(BF16).reshape(nx, part, nz, rows).transpose(2, 0, 1, 3)
    sent = sent.reshape(nz * nx, part, rows)
    got = exchanged(sent, ("z", "x")).reshape(nz, nx, part, rows)

    query_share, grad_share, _ = lax.optimization_barrier(
        ((query_all * share[:, None]).astype(BF16), (grad_all * share[:, None]).astype(BF16), sent)
    )

    def sums_of(grad, weight):
        return jnp.concatenate([dot(grad, query_share, 1, 0), dot(weight, grad_share, 1, 0)], axis=1)

    swap = row_major(sums_of(grad_two, weight_two).astype(BF16))
    swap = shifted(swap, "c", 1)
    mine = row_major((sums_of(grad_one, weight_one) + swap.astype(F32)).astype(BF16))
    got, mine = lax.optimization_barrier((got, mine))
    part_t = got.astype(F32).sum(axis=0)
    part_t = part_t.transpose(1, 0, 2).reshape(part, nx * rows).astype(BF16)
    own, left, right, far = (mine[src // 2 * k : src // 2 * (k + 1)] for k in range(nx))
    own = own.astype(F32)
    moved = [shifted(block, "x", by) for block, by in ((far, 2), (right, 1), (left, -1))]
    for block in moved:
        own = own + block.astype(F32)
    mine = own.astype(BF16)

    def by_core(mine, theirs):
        return jnp.where(core == 0, jnp.stack([mine, theirs]), jnp.stack([theirs, mine]))

    target_all, _ = lax.optimization_barrier((target_all, sent))
    target_other = shifted(target_all, "c", 1)
    target_both = by_core(target_all.T, target_other.T).astype(F32)
    squares = jnp.sum(target_both * target_both, axis=(0, 1))
    high = lax.reduce_precision(squares, 8, 7)
    extra = jnp.stack([high, squares - high]).astype(BF16)
    piece = jnp.concatenate([part_t, extra, jnp.zeros((6, nx * rows), BF16)], axis=0)
    every = told_all(piece, "y").reshape(HEADS // 2, part + 8, nx * rows)
    grad_t = every[:, :part].reshape(HEADS // 2 * part, nx * rows)
    squares_all = every[:, part : part + 2].astype(F32).sum(axis=(0, 1))
    inverse = lax.rsqrt(squares_all / WIDTH + EPS)
    normed_t = (target_both * inverse[None, None]).astype(BF16)
    weight_part = dot(normed_t.reshape(2 * cols, -1), grad_t, 1, 1).astype(BF16)

    weight_sent = weight_part.reshape(2, nz * nx, 8, -1).transpose(1, 0, 2, 3).reshape(nz * nx * 2, 8, -1)
    weight_got = exchanged(weight_sent, ("z", "x", "c"))
    weight_sum = weight_got.reshape(nz, nx * 2, 8, HEADS // 2 * part).astype(F32).sum(axis=0)
    gain_at = (lax.axis_index("z") * nx + x_at) * 8
    weight_sum = weight_sum * lax.dynamic_slice_in_dim(gain, gain_at, 8, 0)[None, :, None]
    weight_sum = lax.optimization_barrier(weight_sum).reshape(nx, 2, 8, HEADS // 2, part)
    grad_weight = weight_sum.transpose(2, 3, 1, 0, 4).reshape(8, WIDTH)

    grad_t, _ = lax.optimization_barrier((grad_t, weight_sent))
    grad_other = shifted(grad_t, "c", 1)
    rows_t = dot(w_mine, grad_t, 1, 0) + dot(w_theirs, grad_other, 1, 0)

    def rows_at(off):
        return lax.dynamic_slice_in_dim(rows_t, lax.rem(x_at + off, nx) * rows, rows, 1)

    rows_sum = rows_at(0)
    for off, by in ((1, 1), (3, -1), (2, 2)):
        rows_sum = rows_sum + shifted(rows_at(off).astype(BF16), "x", by).astype(F32)
    grad_rows = rows_sum.T.astype(BF16)

    mine, _ = lax.optimization_barrier((mine, weight_got))
    sums = exchanged(mine.reshape(ny, bit, 2 * HEAD_DIM), "y")
    sums = sums.reshape(KV_HEADS, 2, bit, 2, HEAD_DIM).astype(F32).sum(axis=1)
    sums = sums.transpose(2, 1, 0, 3).reshape(2, bit, KV_HEADS * HEAD_DIM)
    return (grad_rows, grad_weight, sums[0], sums[1])


def solution(mesh):
    finer = Mesh(mesh.devices.reshape(8, 4, 8, 2), ("z", "x", "y", "c"))
    sp, tp = ("z", "x"), ("y", "c")
    placed = (
        P(sp, tp),
        P(tp),
        P(tp, None),
        P(sp, tp),
        P(sp, None),
        P(sp, None),
        P(sp, tp),
        P(sp, tp),
    )

    return jax.shard_map(
        local,
        mesh=finer,
        in_specs=placed,
        out_specs=(P(sp, tp), P(tp + sp, None), P(sp + tp, None), P(sp + tp, None)),
        check_vma=False,
    )
```

```python
import jax
import jax.numpy as jnp
from jax import lax
from jax.experimental.layout import Layout, with_layout_constraint
from jax.sharding import Mesh
from jax.sharding import PartitionSpec as P

WIDTH = 4096
HEADS = 16
KV_HEADS = 4
HEAD_DIM = 256
EPS = 1e-06
SCALE = HEAD_DIM ** (-0.5)
F32 = jnp.float32
BF16 = jnp.bfloat16


def shifted(value, axis, by):
    n = lax.axis_size(axis)
    return lax.ppermute(value, axis, [(i, (i + by) % n) for i in range(n)])


def exchanged(value, axis):
    return lax.all_to_all(value, axis, split_axis=0, concat_axis=0, tiled=True)


def told_all(value, axis):
    n = lax.axis_size(axis)
    return exchanged(jnp.broadcast_to(value[None], (n, *value.shape)), axis)


def dot(a, b, ca, cb):
    return lax.dot_general(a, b, (((ca,), (cb,)), ((), ())), preferred_element_type=F32)


def row_major(value):
    return with_layout_constraint(value, Layout(major_to_minor=tuple(range(value.ndim))))


def terms(value):
    high = lax.reduce_precision(value, 8, 7)
    rest = value - high
    mid = lax.reduce_precision(rest, 8, 7)
    return [t.astype(BF16) for t in (high, mid, rest - mid)]


def local(target, gain, w_query, queries, keys, values, attn_out, grad_out):
    nz, nx, ny = lax.axis_size("z"), lax.axis_size("x"), lax.axis_size("y")
    rows, cols = queries.shape
    part = cols // nx
    src = keys.shape[0]
    bit = src // (2 * ny)
    core = lax.axis_index("c")
    x_at = lax.axis_index("x")
    kv = lax.axis_index("y") // 2
    n_rows = nz * rows

    delta_own = jnp.sum(attn_out.astype(F32) * grad_out.astype(F32), axis=1)
    line = jnp.concatenate(terms(delta_own) + [jnp.zeros((rows,), BF16)])[None]
    both = jnp.concatenate([queries, grad_out], axis=1)
    both = jnp.concatenate([both, line, jnp.zeros((7, 2 * cols), BF16)], axis=0)
    both = told_all(both, "z")

    def half_of(v):
        v = v.reshape(ny, 2, bit, v.shape[1])
        v = lax.dynamic_slice(v, (0, core, 0, kv * HEAD_DIM), (ny, 1, bit, HEAD_DIM))
        return v.reshape(src // 2, HEAD_DIM)

    pack = row_major(jnp.concatenate([half_of(keys), half_of(values), target], axis=0))
    blocks = [pack] + [shifted(pack, "x", by) for by in (1, -1, 2)]
    target_all = jnp.zeros((nx * rows, cols), BF16)
    for block, off in zip(blocks, (0, 3, 1, 2)):
        target_all = lax.dynamic_update_slice(target_all, block[src:], (lax.rem(x_at + off, nx) * rows, 0))

    w_parts = lax.dynamic_slice(
        w_query.reshape(cols, HEADS // 2, 2, nx, part), (0, 0, 0, x_at, 0), (cols, HEADS // 2, 2, 1, part)
    )
    w_even = w_parts[:, :, 0].reshape(cols, -1)
    w_odd = w_parts[:, :, 1].reshape(cols, -1)
    w_mine = jnp.where(core == 0, w_even, w_odd)
    w_theirs = jnp.where(core == 0, w_odd, w_even)

    half = nx * src // 2
    mine = [b[: src // 2] for b in blocks] + [b[src // 2 : src] for b in blocks]
    mine = row_major(jnp.concatenate(mine, axis=0))
    mine, w_mine, w_theirs = lax.optimization_barrier((mine, w_mine, w_theirs))
    theirs = shifted(mine, "c", 1)
    key_one, value_one = mine[:half], mine[half : 2 * half]
    key_two, value_two = theirs[:half], theirs[half : 2 * half]

    both = both.reshape(nz, rows + 8, 2 * cols)
    query_all = both[:, :rows, :cols].reshape(n_rows, cols)
    grad_all = both[:, :rows, cols:].reshape(n_rows, cols)
    deltas = both[:, rows].astype(F32).reshape(nz, 4, rows).sum(axis=1).reshape(n_rows)
    score_one = dot(key_one, query_all, 1, 1) * SCALE
    score_two = dot(key_two, query_all, 1, 1) * SCALE
    peak = jnp.maximum(jnp.max(score_one, axis=0), jnp.max(score_two, axis=0))
    weight_one = jnp.exp(score_one - peak[None])
    weight_two = jnp.exp(score_two - peak[None])
    total = jnp.sum(weight_one, axis=0) + jnp.sum(weight_two, axis=0)
    weight_one, weight_two, total = lax.optimization_barrier(
        (weight_one.astype(BF16), weight_two.astype(BF16), total)
    )
    stats = told_all(jnp.concatenate([peak, total]).reshape(2 * nz, rows), "z").reshape(nz, 2 * nz, rows)

    def grads_of(weight, value):
        product = dot(value, grad_all, 1, 1)
        return (weight.astype(F32) * ((product - deltas[None]) * SCALE)).astype(BF16)

    grad_one = grads_of(weight_one, value_one)
    grad_two = grads_of(weight_two, value_two)
    query_t = dot(key_one, grad_one, 0, 0) + dot(key_two, grad_two, 0, 0)
    query_t, stats = lax.optimization_barrier((query_t, stats))
    peaks, totals = stats[:, :nz], stats[:, nz:]
    top = jnp.max(peaks, axis=0)
    log_totals = (top + jnp.log(jnp.sum(totals * jnp.exp(peaks - top[None]), axis=0))).reshape(n_rows)
    share = jnp.exp(peak - log_totals)

    sent = (query_t * share[None]).astype(BF16).reshape(nx, part, nz, rows).transpose(2, 0, 1, 3)
    sent = sent.reshape(nz * nx, part, rows)
    got = exchanged(sent, ("z", "x")).reshape(nz, nx, part, rows)

    share, _ = lax.optimization_barrier((share, sent))
    query_share = (query_all * share[:, None]).astype(BF16)
    grad_share = (grad_all * share[:, None]).astype(BF16)

    def sums_of(grad, weight):
        return jnp.concatenate([dot(grad, query_share, 1, 0), dot(weight, grad_share, 1, 0)], axis=1)

    swap = row_major(sums_of(grad_two, weight_two).astype(BF16))
    swap = shifted(swap, "c", 1)
    mine = row_major((sums_of(grad_one, weight_one) + swap.astype(F32)).astype(BF16))
    got, mine = lax.optimization_barrier((got, mine))
    part_t = got.astype(F32).sum(axis=0)
    part_t = part_t.transpose(1, 0, 2).reshape(part, nx * rows).astype(BF16)
    own, left, right, far = (mine[src // 2 * k : src // 2 * (k + 1)] for k in range(nx))
    own = own.astype(F32)
    moved = [shifted(block, "x", by) for block, by in ((far, 2), (right, 1), (left, -1))]
    for block in moved:
        own = own + block.astype(F32)
    mine = own.astype(BF16)

    def by_core(mine, theirs):
        return jnp.where(core == 0, jnp.stack([mine, theirs]), jnp.stack([theirs, mine]))

    target_all, _ = lax.optimization_barrier((target_all, sent))
    target_other = shifted(target_all, "c", 1)
    target_both = by_core(target_all.T, target_other.T).astype(F32)
    squares = jnp.sum(target_both * target_both, axis=(0, 1))
    high = lax.reduce_precision(squares, 8, 7)
    extra = jnp.stack([high, squares - high]).astype(BF16)
    piece = jnp.concatenate([part_t, extra, jnp.zeros((6, nx * rows), BF16)], axis=0)
    every = told_all(piece, "y").reshape(HEADS // 2, part + 8, nx * rows)
    grad_t = every[:, :part].reshape(HEADS // 2 * part, nx * rows)
    squares_all = every[:, part : part + 2].astype(F32).sum(axis=(0, 1))
    inverse = lax.rsqrt(squares_all / WIDTH + EPS)
    normed_t = (target_both * inverse[None, None]).astype(BF16)
    weight_part = dot(normed_t.reshape(2 * cols, -1), grad_t, 1, 1).astype(BF16)

    weight_sent = weight_part.reshape(2, nz * nx, 8, -1).transpose(1, 0, 2, 3).reshape(nz * nx * 2, 8, -1)
    weight_got = exchanged(weight_sent, ("z", "x", "c"))
    weight_sum = weight_got.reshape(nz, nx * 2, 8, HEADS // 2 * part).astype(F32).sum(axis=0)
    gain_at = (lax.axis_index("z") * nx + x_at) * 8
    weight_sum = weight_sum * lax.dynamic_slice_in_dim(gain, gain_at, 8, 0)[None, :, None]
    weight_sum = lax.optimization_barrier(weight_sum).reshape(nx, 2, 8, HEADS // 2, part)
    grad_weight = weight_sum.transpose(2, 3, 1, 0, 4).reshape(8, WIDTH)

    grad_t, _ = lax.optimization_barrier((grad_t, weight_sent))
    grad_other = shifted(grad_t, "c", 1)
    rows_t = dot(w_mine, grad_t, 1, 0) + dot(w_theirs, grad_other, 1, 0)

    def rows_at(off):
        return lax.dynamic_slice_in_dim(rows_t, lax.rem(x_at + off, nx) * rows, rows, 1)

    rows_sum = rows_at(0)
    for off, by in ((1, 1), (3, -1), (2, 2)):
        rows_sum = rows_sum + shifted(rows_at(off).astype(BF16), "x", by).astype(F32)
    grad_rows = rows_sum.T.astype(BF16)

    mine, _ = lax.optimization_barrier((mine, weight_got))
    sums = exchanged(mine.reshape(ny, bit, 2 * HEAD_DIM), "y")
    sums = sums.reshape(KV_HEADS, 2, bit, 2, HEAD_DIM).astype(F32).sum(axis=1)
    sums = sums.transpose(2, 1, 0, 3).reshape(2, bit, KV_HEADS * HEAD_DIM)
    return (grad_rows, grad_weight, sums[0], sums[1])


def solution(mesh):
    finer = Mesh(mesh.devices.reshape(8, 4, 8, 2), ("z", "x", "y", "c"))
    sp, tp = ("z", "x"), ("y", "c")
    placed = (
        P(sp, tp),
        P(tp),
        P(tp, None),
        P(sp, tp),
        P(sp, None),
        P(sp, None),
        P(sp, tp),
        P(sp, tp),
    )

    return jax.shard_map(
        local,
        mesh=finer,
        in_specs=placed,
        out_specs=(P(sp, tp), P(tp + sp, None), P(sp + tp, None), P(sp + tp, None)),
        check_vma=False,
    )
```

```python
import jax
import jax.numpy as jnp
from jax import lax
from jax.experimental.layout import Layout, with_layout_constraint
from jax.sharding import Mesh
from jax.sharding import PartitionSpec as P

WIDTH = 4096
HEADS = 16
KV_HEADS = 4
HEAD_DIM = 256
EPS = 1e-06
SCALE = HEAD_DIM ** (-0.5)
F32 = jnp.float32
BF16 = jnp.bfloat16


def shifted(value, axis, by):
    n = lax.axis_size(axis)
    return lax.ppermute(value, axis, [(i, (i + by) % n) for i in range(n)])


def exchanged(value, axis):
    return lax.all_to_all(value, axis, split_axis=0, concat_axis=0, tiled=True)


def told_all(value, axis):
    n = lax.axis_size(axis)
    return exchanged(jnp.broadcast_to(value[None], (n, *value.shape)), axis)


def dot(a, b, ca, cb):
    return lax.dot_general(a, b, (((ca,), (cb,)), ((), ())), preferred_element_type=F32)


def row_major(value):
    return with_layout_constraint(value, Layout(major_to_minor=tuple(range(value.ndim))))


def terms(value):
    high = lax.reduce_precision(value, 8, 7)
    rest = value - high
    mid = lax.reduce_precision(rest, 8, 7)
    return [t.astype(BF16) for t in (high, mid, rest - mid)]


def local(target, gain, w_query, queries, keys, values, attn_out, grad_out):
    nz, nx, ny = lax.axis_size("z"), lax.axis_size("x"), lax.axis_size("y")
    rows, cols = queries.shape
    part = cols // nx
    src = keys.shape[0]
    bit = src // (2 * ny)
    core = lax.axis_index("c")
    x_at = lax.axis_index("x")
    kv = lax.axis_index("y") // 2
    n_rows = nz * rows

    delta_own = jnp.sum(attn_out.astype(F32) * grad_out.astype(F32), axis=1)
    line = jnp.concatenate(terms(delta_own) + [jnp.zeros((rows,), BF16)])[None]
    both = jnp.concatenate([queries, grad_out], axis=1)
    both = jnp.concatenate([both, line, jnp.zeros((7, 2 * cols), BF16)], axis=0)
    both = told_all(both, "z")

    def half_of(v):
        v = v.reshape(ny, 2, bit, v.shape[1])
        v = lax.dynamic_slice(v, (0, core, 0, kv * HEAD_DIM), (ny, 1, bit, HEAD_DIM))
        return v.reshape(src // 2, HEAD_DIM)

    pack = row_major(jnp.concatenate([half_of(keys), half_of(values), target], axis=0))
    blocks = [pack] + [shifted(pack, "x", by) for by in (1, -1, 2)]
    target_all = jnp.zeros((nx * rows, cols), BF16)
    for block, off in zip(blocks, (0, 3, 1, 2)):
        target_all = lax.dynamic_update_slice(target_all, block[src:], (lax.rem(x_at + off, nx) * rows, 0))

    w_parts = lax.dynamic_slice(
        w_query.reshape(cols, HEADS // 2, 2, nx, part), (0, 0, 0, x_at, 0), (cols, HEADS // 2, 2, 1, part)
    )
    w_even = w_parts[:, :, 0].reshape(cols, -1)
    w_odd = w_parts[:, :, 1].reshape(cols, -1)
    w_mine = jnp.where(core == 0, w_even, w_odd)
    w_theirs = jnp.where(core == 0, w_odd, w_even)

    half = nx * src // 2
    mine = jnp.zeros((2 * half, HEAD_DIM), BF16)
    for k, block in enumerate(blocks):
        mine = lax.dynamic_update_slice(mine, block[: src // 2], (k * src // 2, 0))
        mine = lax.dynamic_update_slice(mine, block[src // 2 : src], (half + k * src // 2, 0))
    mine = row_major(mine)
    mine, w_mine, w_theirs = lax.optimization_barrier((mine, w_mine, w_theirs))
    theirs = shifted(mine, "c", 1)
    key_one, value_one = mine[:half], mine[half : 2 * half]
    key_two, value_two = theirs[:half], theirs[half : 2 * half]

    both = both.reshape(nz, rows + 8, 2 * cols)
    query_all = both[:, :rows, :cols].reshape(n_rows, cols)
    grad_all = both[:, :rows, cols:].reshape(n_rows, cols)
    deltas = both[:, rows].astype(F32).reshape(nz, 4, rows).sum(axis=1).reshape(n_rows)
    score_one = dot(key_one, query_all, 1, 1) * SCALE
    score_two = dot(key_two, query_all, 1, 1) * SCALE
    peak = jnp.maximum(jnp.max(score_one, axis=0), jnp.max(score_two, axis=0))
    weight_one = jnp.exp(score_one - peak[None])
    weight_two = jnp.exp(score_two - peak[None])
    total = jnp.sum(weight_one, axis=0) + jnp.sum(weight_two, axis=0)
    weight_one, weight_two, total = lax.optimization_barrier(
        (weight_one.astype(BF16), weight_two.astype(BF16), total)
    )
    stats = told_all(jnp.concatenate([peak, total]).reshape(2 * nz, rows), "z").reshape(nz, 2 * nz, rows)

    def grads_of(weight, value):
        product = dot(value, grad_all, 1, 1)
        return (weight.astype(F32) * ((product - deltas[None]) * SCALE)).astype(BF16)

    grad_one = grads_of(weight_one, value_one)
    grad_two = grads_of(weight_two, value_two)
    query_t = dot(key_one, grad_one, 0, 0) + dot(key_two, grad_two, 0, 0)
    query_t, stats = lax.optimization_barrier((query_t, stats))
    peaks, totals = stats[:, :nz], stats[:, nz:]
    top = jnp.max(peaks, axis=0)
    log_totals = (top + jnp.log(jnp.sum(totals * jnp.exp(peaks - top[None]), axis=0))).reshape(n_rows)
    share = jnp.exp(peak - log_totals)

    sent = (query_t * share[None]).astype(BF16).reshape(nx, part, nz, rows).transpose(2, 0, 1, 3)
    sent = sent.reshape(nz * nx, part, rows)
    got = exchanged(sent, ("z", "x")).reshape(nz, nx, part, rows)

    share, _ = lax.optimization_barrier((share, sent))
    query_share = (query_all * share[:, None]).astype(BF16)
    grad_share = (grad_all * share[:, None]).astype(BF16)

    def sums_of(grad, weight):
        return jnp.concatenate([dot(grad, query_share, 1, 0), dot(weight, grad_share, 1, 0)], axis=1)

    swap = row_major(sums_of(grad_two, weight_two).astype(BF16))
    swap = shifted(swap, "c", 1)
    mine = row_major((sums_of(grad_one, weight_one) + swap.astype(F32)).astype(BF16))
    got, mine = lax.optimization_barrier((got, mine))
    part_t = got.astype(F32).sum(axis=0)
    part_t = part_t.transpose(1, 0, 2).reshape(part, nx * rows).astype(BF16)
    own, left, right, far = (mine[src // 2 * k : src // 2 * (k + 1)] for k in range(nx))
    own = own.astype(F32)
    moved = [shifted(block, "x", by) for block, by in ((far, 2), (right, 1), (left, -1))]
    for block in moved:
        own = own + block.astype(F32)
    mine = own.astype(BF16)

    def by_core(mine, theirs):
        return jnp.where(core == 0, jnp.stack([mine, theirs]), jnp.stack([theirs, mine]))

    target_all, _ = lax.optimization_barrier((target_all, sent))
    target_other = shifted(target_all, "c", 1)
    target_both = by_core(target_all.T, target_other.T).astype(F32)
    squares = jnp.sum(target_both * target_both, axis=(0, 1))
    high = lax.reduce_precision(squares, 8, 7)
    extra = jnp.stack([high, squares - high]).astype(BF16)
    piece = jnp.concatenate([part_t, extra, jnp.zeros((6, nx * rows), BF16)], axis=0)
    every = told_all(piece, "y").reshape(HEADS // 2, part + 8, nx * rows)
    grad_t = every[:, :part].reshape(HEADS // 2 * part, nx * rows)
    squares_all = every[:, part : part + 2].astype(F32).sum(axis=(0, 1))
    inverse = lax.rsqrt(squares_all / WIDTH + EPS)
    normed_t = (target_both * inverse[None, None]).astype(BF16)
    weight_part = dot(normed_t.reshape(2 * cols, -1), grad_t, 1, 1).astype(BF16)

    weight_sent = weight_part.reshape(2, nz * nx, 8, -1).transpose(1, 0, 2, 3).reshape(nz * nx * 2, 8, -1)
    weight_got = exchanged(weight_sent, ("z", "x", "c"))
    weight_sum = weight_got.reshape(nz, nx * 2, 8, HEADS // 2 * part).astype(F32).sum(axis=0)
    gain_at = (lax.axis_index("z") * nx + x_at) * 8
    weight_sum = weight_sum * lax.dynamic_slice_in_dim(gain, gain_at, 8, 0)[None, :, None]
    weight_sum = lax.optimization_barrier(weight_sum).reshape(nx, 2, 8, HEADS // 2, part)
    grad_weight = weight_sum.transpose(2, 3, 1, 0, 4).reshape(8, WIDTH)

    grad_t, _ = lax.optimization_barrier((grad_t, weight_sent))
    grad_other = shifted(grad_t, "c", 1)
    rows_t = dot(w_mine, grad_t, 1, 0) + dot(w_theirs, grad_other, 1, 0)

    def rows_at(off):
        return lax.dynamic_slice_in_dim(rows_t, lax.rem(x_at + off, nx) * rows, rows, 1)

    rows_sum = rows_at(0)
    for off, by in ((1, 1), (3, -1), (2, 2)):
        rows_sum = rows_sum + shifted(rows_at(off).astype(BF16), "x", by).astype(F32)
    grad_rows = rows_sum.T.astype(BF16)

    mine, _ = lax.optimization_barrier((mine, weight_got))
    sums = exchanged(mine.reshape(ny, bit, 2 * HEAD_DIM), "y")
    sums = sums.reshape(KV_HEADS, 2, bit, 2, HEAD_DIM).astype(F32).sum(axis=1)
    sums = sums.transpose(2, 1, 0, 3).reshape(2, bit, KV_HEADS * HEAD_DIM)
    return (grad_rows, grad_weight, sums[0], sums[1])


def solution(mesh):
    finer = Mesh(mesh.devices.reshape(8, 4, 8, 2), ("z", "x", "y", "c"))
    sp, tp = ("z", "x"), ("y", "c")
    placed = (
        P(sp, tp),
        P(tp),
        P(tp, None),
        P(sp, tp),
        P(sp, None),
        P(sp, None),
        P(sp, tp),
        P(sp, tp),
    )

    return jax.shard_map(
        local,
        mesh=finer,
        in_specs=placed,
        out_specs=(P(sp, tp), P(tp + sp, None), P(sp + tp, None), P(sp + tp, None)),
        check_vma=False,
    )
```
